512 devices in a mesh: sp: 32 (over z, core), tp: 16 (over y, x).
Axes of the slice: x: 4, y: 4, z: 16, core: 2. Of those that a mesh axis runs over, the one named last changes fastest.
Arguments:
- residual_in: bfloat16 [8192, 2048], P('sp', 'tp'), may hold values from -20 to 20
- conv_value: bfloat16 [8192, 2048], P('sp', 'tp'), may hold values from -6 to 6
- conv_gate: bfloat16 [8192, 2048], P('sp', 'tp'), may hold values from -9 to 9
- doc_ids: int32 [8192], P('sp'), may hold values from 0 to 15, never falling along the last dimension, each value on 1 to 1024 neighbouring positions
- conv_kernel: bfloat16 [31, 2048], P(None, 'tp'), may hold values from -3 to 3
- ln_gain: bfloat16 [2048], P('tp'), may hold values from 0.099609375 to 1.8984375
- out_weight: bfloat16 [2048, 2048], P(None, 'tp'), may hold values from -0.25 to 0.25
- norm_gain: bfloat16 [2048], P('tp'), may hold values from 0.099609375 to 1.8984375
- routes: int32 [8192, 2], P('sp'), may hold values from 0 to 31, all different within a row; in each aligned block of 256 rows (0 to 255, 256 to 511, ...) at most 32 rows name the same one
- route_weight: float32 [8192, 2], P('sp'), may hold values from 0.1 to 1
- gate_w: bfloat16 [32, 2048, 4096], P('sp', None, 'tp'), may hold values from -0.125 to 0.125
- up_w: bfloat16 [32, 2048, 4096], P('sp', None, 'tp'), may hold values from -0.125 to 0.125
- down_w: bfloat16 [32, 4096, 2048], P('sp', 'tp'), may hold values from -0.125 to 0.125
Outputs:
- mixed: bfloat16 [8192, 2048], P('sp', 'tp')
The draws below stay inside these ranges and needn't reach their ends.
Inputs may be any that keep to these rules, and one draw needn't show every extreme that they name: `routes`: in each aligned block of 256 positions no expert is named by more than 32 positions, a bound that some block reaches; a position's two experts differ. `doc_ids`: never falls along the positions; each document spans 1 to 1024 positions, one exactly that many.
All inputs are finite; a program needn't handle non-finite values.
Results may differ from the reference program's by a relative error of at most 0.012.
Values may be sent and summed in bfloat16 or wider, within the bound.
A program may use at most 64 MiB of HBM per device.

```python
import math
import jax
import jax.numpy as jnp
import numpy as np
from jax import lax

D = 2048
C = 2048
FE = 4096
KW = 31
TOK_SP = 256
TOKENS = 8192
EXPERTS = 32
CAP = 32
N_SP = 32
N_TP = 16


def draw_residual_in(key, part):
    column = jnp.arange(D, dtype=jnp.float32) / D
    scale = 0.3 * 10.0 ** column
    base = jnp.clip(jax.random.normal(key, (TOKENS, D), jnp.float32), -6.0, 6.0)
    return (base * scale).astype(jnp.bfloat16)


def draw_conv_kernel(key, part):
    channel = jnp.arange(C, dtype=jnp.float32) / C
    scale = KW ** (-0.5) * 10.0 ** channel / 3.0
    base = jnp.clip(jax.random.normal(key, (KW, C), jnp.float32), -4.0, 4.0)
    return (base * scale).astype(jnp.bfloat16)


def strengthened(array, own_key, source, target, blocks, factor):
    owner, partner = [(jnp.arange(array.shape[dim]) // (array.shape[dim] // blocks)).reshape([-1 if axis == dim else 1 for axis in range(array.ndim)]) for dim in (source, target)]
    chosen = jax.random.permutation(own_key, blocks)[partner]
    strong = (owner == chosen) | (owner == (partner + blocks // 2) % blocks)
    return jnp.where(strong, factor * array, array)


def levels(own_key, extent, shards, least, top_value):
    def one(dim, shards_of):
        heights = jax.random.uniform(jax.random.fold_in(jax.random.fold_in(own_key, 6), dim), (shards_of,), jnp.float32, least / len(shards), top_value / len(shards))
        return jnp.repeat(jnp.exp(heights), extent[dim] // shards_of).reshape((-1,) + (1,) * (len(extent) - dim - 1))

    gain = one(*shards[0])
    for cut in shards[1:]:
        gain = gain * one(*cut)
    return gain


def length_profile(amount, total, bound, skew):
    portions = [(1 << 20) // math.isqrt(grade ** skew) + 1 for grade in range(2, amount + 1)]
    spare, given = total - bound - (amount - 1), [1] * (amount - 1)
    while spare > 0:
        free = [i for i in range(amount - 1) if given[i] < bound]
        whole, left = sum([portions[i] for i in free]), spare
        for i in free:
            extra = min(bound - given[i], max(1, left * portions[i] // whole), spare)
            given[i] = given[i] + extra
            spare = spare - extra
    return np.array([bound] + given)


def uneven(stream_key, amount, total, bound, lean):
    if amount == 2:
        one = jax.random.randint(stream_key, (), max(1, total - bound), min(bound, total - 1) + 1)
        return jnp.stack([one, total - one])
    tallies = jnp.asarray(length_profile(amount, total, bound, lean), jnp.int32)
    couples = (amount - 1) // 2
    source_of, receiver = tallies[1:1 + 2 * couples:2], tallies[2:2 + 2 * couples:2]
    room = jnp.minimum(source_of - 1, bound - receiver)
    passed = jax.random.randint(jax.random.fold_in(stream_key, 1), (couples,), 0, 1 << 20) % (room + 1)
    tallies = tallies.at[1:1 + 2 * couples:2].set(source_of - passed).at[2:2 + 2 * couples:2].set(receiver + passed)
    return tallies[jax.random.permutation(jax.random.fold_in(stream_key, 2), amount)]


def routed_block(key, own, number, rows, number_of, top, most, lean):
    ranking = jax.random.permutation(key, number_of)
    crowded, usual = shares(number_of, rows * top, most, lean, True), shares(number_of, rows * top, most, lean, False)
    places = jnp.arange(number_of)

    def named(sizes, turn):
        used = int((sizes > 0).sum())
        fixed = max(1, used // 4)
        shifted = fixed + (places - fixed + turn * (used - fixed)) % max(1, number_of - fixed)
        return jnp.zeros((number_of,), jnp.int32).at[ranking[jnp.where(places < fixed, places, shifted)]].set(jnp.asarray(sizes, jnp.int32))

    sizes = jnp.where(number % 4 == 0, named(crowded, number // 4), named(usual, number - number // 4 - 1))
    mixed = jax.random.permutation(jax.random.fold_in(own, 3), number_of)
    source_of, receiver = mixed[0:number_of // 2 * 2:2], mixed[1:number_of // 2 * 2:2]
    margin = jnp.minimum(sizes[source_of] - 1, most - sizes[receiver]) // 2
    margin = jnp.where((source_of == ranking[0]) | (receiver == ranking[0]) | (sizes[receiver] == 0), 0, jnp.maximum(margin, 0))
    shifted = jax.random.randint(jax.random.fold_in(own, 4), (number_of // 2,), 0, 1 << 20) % (margin + 1)
    sizes = sizes.at[source_of].add(-shifted).at[receiver].add(shifted)
    labels = jnp.searchsorted(jnp.cumsum(sizes), jnp.arange(rows * top), side="right").astype(jnp.int32)
    listing = labels.reshape(top, rows).T
    listing = listing[jax.random.permutation(jax.random.fold_in(own, 1), rows)]
    turn = jax.random.randint(jax.random.fold_in(own, 2), (rows, 1), 0, top)
    return jnp.take_along_axis(listing, (jnp.arange(top)[None, :] + turn) % top, axis=1)


def shares(amount, total, reach, lean, full):
    weights = [(1 << 20) // math.isqrt(grade ** lean) + 1 for grade in range(1, amount + 1)]
    largest = reach if full else min(reach, max(-(-total // amount), total * weights[0] // sum(weights)))
    least = 1 if total - largest >= amount - 1 else 0
    counts, rest = [largest] + [least] * (amount - 1), total - largest - least * (amount - 1)
    while rest > 0:
        movable = [i for i in range(1, amount) if counts[i] < largest] or [i for i in range(1, amount) if counts[i] < reach]
        mass, remaining = sum([weights[i] for i in movable]), rest
        for i in movable:
            more = min(reach - counts[i], max(1, remaining * weights[i] // mass), rest)
            counts[i] = counts[i] + more
            rest = rest - more
    return np.array(counts)


def scatter_about(stream_key, dims, width, most, cuts=(), kind=jnp.bfloat16):
    gain = levels(stream_key, dims, cuts, -0.22, 0.18) if cuts else 1.0
    drawn = jax.random.normal(stream_key, dims, jnp.float32) * width * gain
    return jnp.minimum(jnp.maximum(drawn, -most), most).astype(kind)


def bell_draw_with(own_key, dims, deviation, reach, pieces, heavy, kind=jnp.bfloat16):
    drawn = deviation * jax.random.normal(own_key, dims, jnp.float32)
    if pieces:
        drawn = drawn * levels(own_key, dims, pieces, -0.22, 0.18)
    return jnp.clip(strengthened(drawn, jax.random.fold_in(own_key, 3), *heavy), -reach, reach).astype(kind)


def setup_inputs(seed: int = 0) -> dict:
    key_list = jax.random.split(jax.random.key(seed), 14)
    residual_in = draw_residual_in(jax.random.fold_in(key_list[13], 71), 0)
    conv_value = scatter_about(key_list[1], (TOKENS, C), 1.0, 6.0, ((0, 32), (1, 16)))
    conv_gate = scatter_about(key_list[2], (TOKENS, C), 1.5, 9.0, ((0, 32), (1, 16)))
    doc_ids = jnp.searchsorted(jnp.cumsum(uneven(key_list[3], N_SP // 2, TOKENS, 4 * TOK_SP, 0)), jnp.arange(TOKENS), side="right").astype(jnp.int32)
    conv_kernel = draw_conv_kernel(jax.random.fold_in(key_list[13], 71), 0)
    ln_gain = jnp.clip(1.0 + 0.18 * jax.random.normal(key_list[5], (C,), jnp.float32), 0.099609375, 1.8984375).astype(jnp.bfloat16)
    out_weight = scatter_about(key_list[6], (C, D), (C // 4) ** -0.5, 0.25, ((1, 16),))
    norm_gain = jnp.clip(1.0 + 0.18 * jax.random.normal(key_list[7], (D,), jnp.float32), 0.099609375, 1.8984375).astype(jnp.bfloat16)
    routes_keys = jax.random.split(jax.random.fold_in(key_list[8], 1), TOKENS // TOK_SP)
    routes_turns = jax.random.permutation(jax.random.fold_in(key_list[8], 3), TOKENS // TOK_SP)
    routes = jax.vmap(lambda own, number: routed_block(jax.random.fold_in(key_list[8], 2), own, number, TOK_SP, EXPERTS, 2, CAP, 1))(routes_keys, routes_turns).reshape((TOKENS, 2))
    route_weight = jnp.clip(jnp.exp(math.log(1.0) - 2.3025851 * jax.random.uniform(key_list[9], (TOKENS, 2), jnp.float32) ** levels(key_list[9], (TOKENS, 2), ((0, 32),), -0.2, 0.2)), 0.1, 1.0)
    gate_w = scatter_about(key_list[10], (EXPERTS, D, FE), D ** -0.5, 0.125, ((0, 32), (2, 16)))
    up_w = scatter_about(key_list[11], (EXPERTS, D, FE), D ** -0.5, 0.125, ((0, 32), (2, 16)))
    down_w = bell_draw_with(key_list[12], (EXPERTS, FE, D), FE ** -0.5, 0.125, ((0, 32), (1, 16)), (1, 2, 16, 2.0))
    return {"residual_in": residual_in, "conv_value": conv_value, "conv_gate": conv_gate, "doc_ids": doc_ids, "conv_kernel": conv_kernel, "ln_gain": ln_gain, "out_weight": out_weight, "norm_gain": norm_gain, "routes": routes, "route_weight": route_weight, "gate_w": gate_w, "up_w": up_w, "down_w": down_w}


epsilon = 1e-06

def reference(residual_in, conv_value, conv_gate, doc_ids, conv_kernel, ln_gain, out_weight, norm_gain, routes, route_weight, gate_w, up_w, down_w):
    gated = (conv_value.astype(jnp.float32) * jax.nn.sigmoid(conv_gate.astype(jnp.float32))).astype(jnp.bfloat16)
    positions = gated.shape[0]
    lookback = KW - 1
    padded = jnp.concatenate([jnp.zeros((lookback, C), jnp.bfloat16), gated], 0)
    doc_padded = jnp.concatenate([jnp.full((lookback,), -1, jnp.int32), doc_ids], 0)
    kernel = conv_kernel.astype(jnp.float32)
    conv_out = jnp.zeros((positions, C), jnp.float32)
    for kernel_tap in range(KW):
        same_doc = (doc_padded[kernel_tap:kernel_tap + positions] == doc_ids)[:, None]
        conv_out = conv_out + jnp.where(same_doc, padded[kernel_tap:kernel_tap + positions].astype(jnp.float32) * kernel[kernel_tap], 0.0)
    chan_mean = lax.optimization_barrier(jnp.mean(conv_out, 1, keepdims=True))
    chan_square = lax.optimization_barrier(jnp.mean(conv_out * conv_out, 1, keepdims=True))
    activated = jax.nn.silu((conv_out - chan_mean) * lax.rsqrt(chan_square - chan_mean * chan_mean + epsilon) * ln_gain.astype(jnp.float32)).astype(jnp.bfloat16)
    projected = jnp.dot(activated, out_weight, preferred_element_type=jnp.float32).astype(jnp.bfloat16)
    stream = (residual_in.astype(jnp.float32) + projected.astype(jnp.float32)).astype(jnp.bfloat16)
    stream_f = stream.astype(jnp.float32)
    normed = (stream_f * lax.rsqrt(lax.optimization_barrier(jnp.mean(stream_f * stream_f, 1, keepdims=True)) + epsilon) * norm_gain.astype(jnp.float32)).astype(jnp.bfloat16)
    capacity = 4 * TOK_SP // EXPERTS
    flat_routes = routes.reshape(N_SP, TOK_SP * 2)
    onehot = (flat_routes[:, :, None] == jnp.arange(EXPERTS, dtype=jnp.int32)).astype(jnp.int32)
    slot_rank = lax.optimization_barrier(jnp.sum((jnp.cumsum(onehot, 1) - onehot) * onehot, 2)).astype(jnp.int32)
    token_local = jnp.arange(TOK_SP * 2, dtype=jnp.int32) // 2
    block_start = (jnp.arange(N_SP, dtype=jnp.int32) * TOK_SP)[:, None]
    token_global = token_local[None, :] + block_start
    slot_token = jnp.full((N_SP, EXPERTS * capacity), positions, jnp.int32)
    slot_token = slot_token.at[jnp.arange(N_SP, dtype=jnp.int32)[:, None], flat_routes * capacity + slot_rank].set(token_global)
    slot_token = slot_token.reshape(N_SP, EXPERTS, capacity).transpose(1, 0, 2).reshape(EXPERTS, N_SP * capacity)

    def expert(operands):
        chosen, weight_gate, weight_up, weight_down = operands
        gathered = jnp.take(normed, chosen, axis=0, mode='fill', fill_value=0)
        hidden = (jax.nn.silu(jnp.dot(gathered, weight_gate, preferred_element_type=jnp.float32)) * jnp.dot(gathered, weight_up, preferred_element_type=jnp.float32)).astype(jnp.bfloat16)
        blocks = hidden.reshape(-1, N_TP, FE // N_TP).astype(jnp.float32)
        partials = jnp.einsum('rnf,nfd->nrd', blocks, weight_down.reshape(N_TP, FE // N_TP, D).astype(jnp.float32))
        partials = lax.optimization_barrier(partials.astype(jnp.bfloat16)).astype(jnp.float32)
        return lax.optimization_barrier(jnp.sum(partials, 0)).astype(jnp.bfloat16)
    expert_out = lax.map(expert, (slot_token, gate_w, up_w, down_w))
    source_row = jnp.arange(N_SP, dtype=jnp.int32)[:, None] * capacity
    pick_index = (flat_routes * (N_SP * capacity) + source_row + slot_rank).reshape(-1)
    picked = jnp.take(expert_out.reshape(-1, D), pick_index, axis=0).reshape(positions, 2, D)
    routed = lax.optimization_barrier(jnp.sum(picked.astype(jnp.float32) * route_weight[:, :, None], 1))
    return (stream_f + routed).astype(jnp.bfloat16)
```

```python
import functools

import jax
import jax.numpy as jnp
from jax import lax
from jax.experimental import pallas as pl
from jax.experimental.pallas import tpu as pltpu
from jax.sharding import Mesh
from jax.sharding import PartitionSpec as P

MESH = pl.DeviceIdType.MESH
F32 = jnp.float32
BF16 = jnp.bfloat16
AXES = ("z", "core", "y", "x")
TP = ("y", "x")
SP = ("z", "core")
EPS = 1e-06

ROWS = 256
LANES = 128
RING = 4
NTP = RING * RING
WIDE = RING * LANES
FULL = NTP * LANES
TAPS = 31
HALO = 32
EXPERTS = 32
CAP = 32
SLOTS = EXPERTS * CAP
NZ = 16
G1 = 2
G2 = 4
R1 = ROWS // G1 // 2
R2 = SLOTS // G2 // 2
CHUNKS = R2 // CAP
ZFIRST = 4


def remote(src, dst, send, recv, dev):
    return pltpu.make_async_remote_copy(
        src_ref=src,
        dst_ref=dst,
        send_sem=send,
        recv_sem=recv,
        device_id=dev,
        device_id_type=MESH,
    )


def distance(i):
    k = lax.rem(i + ZFIRST, NZ)
    half = (k + 1) // 2
    return jnp.where(lax.rem(k, 2) == 1, half, NZ - half)


def to_column(row):
    return jnp.transpose(jnp.broadcast_to(row, (LANES, row.shape[1])))


def true_block(part, pos):
    return pos if part == 0 else (pos % RING) * RING + pos // RING


def kernel(
    cv,
    cg,
    doc,
    ck,
    lng,
    res,
    routes,
    rw,
    ng,
    ow_hbm,
    gw_hbm,
    uw_hbm,
    dw_hbm,
    out,
    ow,
    gw,
    uw,
    dw,
    ext,
    docx,
    hg_out,
    hd_out,
    hg_in,
    hd_in,
    conv,
    stat,
    gains,
    colstat,
    xg,
    act,
    strm,
    pick,
    dsp,
    x2g,
    nrm,
    hid,
    part_sum,
    t1,
    u1,
    v1,
    s1,
    q1,
    t2,
    u2,
    v2,
    s2,
    fin,
    ret,
    wsem,
    hsend,
    hrecv,
    stsend,
    strecv,
    ssem1,
    rsem1,
    ssem2,
    rsem2,
    dsend,
    drecv,
    rsend,
    rrecv,
):
    z = lax.axis_index("z")
    c = lax.axis_index("core")
    y = lax.axis_index("y")
    x = lax.axis_index("x")
    me_tp = y * RING + x
    me_sp = z * 2 + c

    weights = [
        pltpu.make_async_copy(src, dst, wsem.at[i])
        for i, (src, dst) in enumerate(
            ((ow_hbm, ow), (gw_hbm.at[0], gw), (uw_hbm.at[0], uw), (dw_hbm.at[0], dw))
        )
    ]
    for w in weights:
        w.start()

    barrier = pltpu.get_barrier_semaphore()

    def tp_peer(k):
        other = lax.rem(me_tp + k, NTP)
        return (z, c, other // RING, lax.rem(other, RING))

    def sp_peer(k):
        other = lax.rem(me_sp + k, 2 * NZ)
        return (other // 2, lax.rem(other, 2), y, x)

    def greet_tp(k, carry):
        pl.semaphore_signal(barrier, inc=1, device_id=tp_peer(k), device_id_type=MESH)
        return carry

    def greet_sp(k, carry):
        pl.semaphore_signal(barrier, inc=1, device_id=sp_peer(k), device_id_type=MESH)
        return carry

    lax.fori_loop(1, 2 * NZ, greet_sp, 0)
    lax.fori_loop(1, NTP, greet_tp, 0)

    gate = cg[...].astype(F32)
    gated = (cv[...].astype(F32) * (1.0 / (1.0 + jnp.exp(-gate)))).astype(BF16)
    ext[HALO:, :] = gated.astype(F32)
    hg_out[...] = gated[ROWS - HALO :, :]
    dcol = to_column(doc[...].astype(F32))
    docx[HALO:, :] = dcol
    hd_out[...] = dcol[ROWS - HALO :, :]
    taps = ck[...].astype(F32)

    def conv_rows(first, count):
        acc = jnp.zeros((count, LANES), F32)
        mine = docx[HALO + first : HALO + first + count, :]
        for tap in range(TAPS):
            at = HALO + first - (TAPS - 1) + tap
            same = docx[at : at + count, :] == mine
            term = ext[at : at + count, :] * taps[tap : tap + 1, :]
            acc = acc + jnp.where(same, term, 0.0)
        conv[first : first + count, :] = acc

    for first in range(HALO, ROWS, 32):
        conv_rows(first, 32)

    pl.semaphore_wait(barrier, NTP - 1 + 2 * NZ - 1)

    after = sp_peer(1)
    halo_g = remote(hg_out, hg_in, hsend.at[0], hrecv.at[0], after)
    halo_d = remote(hd_out, hd_in, hsend.at[1], hrecv.at[1], after)
    halo_g.start()
    halo_d.start()

    ids = routes[...]
    expert = lax.broadcasted_iota(jnp.int32, (EXPERTS, ROWS), 0)
    names = [(expert == ids[k : k + 1, :]).astype(F32) for k in range(2)]
    before = (
        lax.broadcasted_iota(jnp.int32, (ROWS, ROWS), 0)
        < lax.broadcasted_iota(jnp.int32, (ROWS, ROWS), 1)
    ).astype(F32)
    earlier = jnp.dot(
        (names[0] + names[1]).astype(BF16), before.astype(BF16), preferred_element_type=F32
    )
    slot_base = expert.astype(F32) * float(CAP)
    slots = [jnp.sum(n * (earlier + slot_base), axis=0, keepdims=True) for n in names]
    lane = lax.broadcasted_iota(jnp.int32, (ROWS, LANES), 1).astype(F32)
    for k in range(2):
        col = to_column(slots[k])
        for b in range(SLOTS // LANES):
            pick[k, :, b * LANES : (b + 1) * LANES] = (
                (lane + float(b * LANES)) == col
            ).astype(BF16)

    halo_g.wait()
    halo_d.wait()
    first_block = me_sp == 0
    ext[:HALO, :] = hg_in[...].astype(F32)
    docx[:HALO, :] = jnp.where(first_block, -1.0, hd_in[...])
    conv_rows(0, HALO)

    cx = conv[...]
    cxt = jnp.transpose(cx)
    local = jnp.sum(cxt, axis=0, keepdims=True) * (1.0 / LANES)
    spread = cxt - local
    second = jnp.sum(spread * spread, axis=0, keepdims=True)
    gain_row = jnp.concatenate([lng[...].astype(F32), ng[...].astype(F32)], axis=1)
    stat[me_tp] = jnp.concatenate(
        [local, second, gain_row, jnp.zeros((5, ROWS), F32)], axis=0
    )
    dev = (cx - to_column(local)).astype(BF16)
    for g in range(G1):
        for part in range(2):
            mm, mj = (x, y) if part == 0 else (y, x)
            lo = g * 2 * R1 + part * R1
            pos = pl.multiple_of((mj * RING + mm) * LANES, LANES)
            xg[lo : lo + R1, pl.ds(pos, LANES)] = dev[lo : lo + R1, :]

    def send_stat(k, carry):
        remote(stat.at[me_tp], stat.at[me_tp], stsend.at[k], strecv.at[k], tp_peer(k)).start()
        return carry

    def ring(part, g, rows, first):
        mm, mj = (x, y) if part == 0 else (y, x)
        step = 1 - 2 * (g % 2) if isinstance(g, int) else 1 - 2 * lax.rem(g, 2)

        def at(base, by):
            return lax.rem(base + by * step + 2 * RING, RING)

        def minor(by):
            m = at(mm, by)
            return (z, c, mj, m) if part == 0 else (z, c, m, mj)

        def major(by):
            m = at(mj, by)
            return (z, c, m, mm) if part == 0 else (z, c, mm, m)

        def block(by):
            return pl.ds(pl.multiple_of((mj * RING + at(mm, by)) * LANES, LANES), LANES)

        def wide(by):
            return pl.ds(pl.multiple_of(at(mj, by) * WIDE, WIDE), WIDE)

        def small(by):
            return pl.ds(pl.multiple_of(at(mm, by) * LANES, LANES), LANES)

        lo = pl.multiple_of(first(g, part), rows)
        return minor, major, block, wide, small, pl.ds(lo, rows)

    def make_gather(buf, rows, first, ssem, rsem):
        def move(g, part, kind, cols, dev):
            r = pl.ds(pl.multiple_of(first(g, part), rows), rows)
            ref = buf.at[r, cols]
            return remote(ref, ref, ssem.at[part, kind], rsem.at[g, part, kind], dev)

        def send(g, part, kind, cols, dev):
            d = move(g, part, kind, cols, dev)

            if isinstance(g, int):
                if g > 0:
                    d.wait_send()
            else:
                pl.when(g > 0)(d.wait_send)
            d.start()

        def s0(g):
            for part in range(2):
                minor, _, block, _, _, _ = ring(part, g, rows, first)
                send(g, part, 0, block(0), minor(1))
                send(g, part, 1, block(0), minor(-1))

        def s1(g):
            for part in range(2):
                minor, _, block, _, _, _ = ring(part, g, rows, first)
                move(g, part, 0, block(-1), minor(1)).wait_recv()
                send(g, part, 2, block(-1), minor(1))

        def s2(g):
            for part in range(2):
                minor, major, block, wide, _, _ = ring(part, g, rows, first)
                move(g, part, 1, block(1), minor(1)).wait_recv()
                move(g, part, 2, block(2), minor(1)).wait_recv()
                send(g, part, 3, wide(0), major(1))
                send(g, part, 4, wide(0), major(-1))

        def s3(g):
            for part in range(2):
                _, major, _, wide, _, _ = ring(part, g, rows, first)
                move(g, part, 3, wide(-1), major(1)).wait_recv()
                send(g, part, 5, wide(-1), major(1))

        def s4(g):
            for part in range(2):
                _, major, _, wide, _, _ = ring(part, g, rows, first)
                move(g, part, 4, wide(1), major(1)).wait_recv()
                move(g, part, 5, wide(2), major(1)).wait_recv()

        def drain():
            for part in range(2):
                minor, major, block, wide, _, _ = ring(part, 0, rows, first)
                for kind in range(3):
                    move(0, part, kind, block(0), minor(1)).wait_send()
                for kind in range(3, 6):
                    move(0, part, kind, wide(0), major(1)).wait_send()

        return s0, s1, s2, s3, s4, drain

    def pipeline(stages, groups):
        last = max(d for d, _ in stages)

        def step(t, carry):
            for delay, stage in stages:
                g = t - delay

                @pl.when((g >= 0) & (g < groups))
                def _(stage=stage, g=g):
                    stage(g)

            return carry

        lax.fori_loop(0, groups + last, step, 0)

    def first1(g, part):
        return g * 2 * R1 + part * R1

    a0, a1, a2, a3, a4, adrain = make_gather(xg, R1, first1, ssem1, rsem1)
    for g in range(G1):
        a0(g)
    lax.fori_loop(1, NTP, send_stat, 0)
    pipeline(((4, a4), (3, a3), (2, a2), (1, a1)), G1)

    def wait_stat(k, carry):
        d = remote(stat.at[me_tp], stat.at[me_tp], stsend.at[k], strecv.at[k], tp_peer(k))
        d.wait_send()
        d.wait_recv()
        return carry

    lax.fori_loop(1, NTP, wait_stat, 0)
    adrain()

    means = [stat[j, 0:1, :] for j in range(NTP)]
    mean = sum(means) * (1.0 / NTP)
    shifts = [m - mean for m in means]
    var = (
        sum(stat[j, 1:2, :] for j in range(NTP)) * (1.0 / FULL)
        + sum(s * s for s in shifts) * (1.0 / NTP)
    )
    scale = lax.rsqrt(var + EPS)
    table = jnp.concatenate(shifts + [scale] + [jnp.zeros((LANES - NTP - 1, ROWS), F32)], axis=0)
    colstat[...] = jnp.transpose(table)
    for j in range(NTP):
        gains[:, j * LANES : (j + 1) * LANES] = jnp.concatenate(
            [stat[j, 2:3, :LANES], stat[j, 2:3, LANES:], jnp.zeros((6, LANES), F32)], axis=0
        )

    for part in range(2):

        def normalise(i, carry, part=part):
            g = i // (R1 // 16)
            lo = pl.multiple_of(first1(g, part) + lax.rem(i, R1 // 16) * 16, 16)
            cs = colstat[pl.ds(lo, 16), :]
            rs = cs[:, NTP : NTP + 1]
            for pos in range(NTP):
                j = true_block(part, pos)
                v = xg[pl.ds(lo, 16), pos * LANES : (pos + 1) * LANES].astype(F32)
                v = (v + cs[:, j : j + 1]) * rs * gains[0:1, j * LANES : (j + 1) * LANES]
                v = v / (1.0 + jnp.exp(-v))
                act[pl.ds(lo, 16), j * LANES : (j + 1) * LANES] = v.astype(BF16)
            return carry

        lax.fori_loop(0, G1 * R1 // 16, normalise, 0)

    weights[0].wait()
    projected = jnp.dot(act[...], ow[...], preferred_element_type=F32).astype(BF16)
    strm[...] = (res[...].astype(F32) + projected.astype(F32)).astype(BF16)

    slot = lax.broadcasted_iota(jnp.int32, (SLOTS, ROWS), 0).astype(F32)
    chosen = ((slot == slots[0]) | (slot == slots[1])).astype(BF16)
    dsp[...] = (
        jnp.dot(chosen, strm[...], preferred_element_type=F32)
        .astype(BF16)
        .reshape(EXPERTS, CAP, LANES)
    )

    pos_a = pl.multiple_of((y * RING + x) * LANES, LANES)
    pos_b = pl.multiple_of((x * RING + y) * LANES, LANES)

    def own_pos(r):
        return pl.multiple_of(jnp.where(lax.rem(r // CHUNKS, 2) == 0, pos_a, pos_b), LANES)

    r_self = ((NZ - ZFIRST) % NZ) * 2
    g_self, part_self = r_self // (2 * CHUNKS), (r_self // CHUNKS) % 2

    def dispatch(r, turn):
        dz = distance(r // 2)
        zt = lax.rem(z - dz + NZ, NZ)
        ct = lax.rem(c + r, 2)
        lo = pl.multiple_of(r * CAP, CAP)
        return remote(
            dsp.at[zt * 2 + ct],
            x2g.at[pl.ds(lo, CAP), pl.ds(own_pos(r), LANES)],
            dsend,
            drecv.at[r // CHUNKS],
            (zt, ct, y, x),
        )

    def send_dispatch(r, carry):
        @pl.when(r != r_self)
        def _():
            dispatch(r, 0).start()

        return carry

    lax.fori_loop(0, EXPERTS, send_dispatch, 0)
    x2g[r_self * CAP : (r_self + 1) * CAP, pl.ds(own_pos(jnp.int32(r_self)), LANES)] = dsp[me_sp]

    def first2(g, part):
        return g * 2 * R2 + part * R2

    b0, b1, b2, b3, b4, bdrain = make_gather(x2g, R2, first2, ssem2, rsem2)

    def arrivals(g):
        for part in range(2):
            pos = pos_a if part == 0 else pos_b
            lo = pl.multiple_of(first2(g, part), R2)
            sem = drecv.at[g * 2 + part]
            full = x2g.at[pl.ds(lo, R2), pl.ds(pos, LANES)]
            less = x2g.at[pl.ds(lo, R2 - CAP), pl.ds(pos, LANES)]
            if part == part_self:

                @pl.when(g == g_self)
                def _():
                    pltpu.make_async_copy(less, less, sem).wait()

                @pl.when(g != g_self)
                def _():
                    pltpu.make_async_copy(full, full, sem).wait()
            else:
                pltpu.make_async_copy(full, full, sem).wait()

    def first_stage(g):
        arrivals(g)
        b0(g)

    for w in weights[1:]:
        w.wait()

    def exchange(g, part, kind, src, dst, dev):
        return remote(src, dst, ssem2.at[part, kind], rsem2.at[g, part, kind], dev)

    def push(g, d):
        @pl.when(g > 0)
        def _():
            d.wait_send()

        d.start()

    def expert_stage(g):
        b4(g)
        base = pl.multiple_of(g * 2 * R2, 2 * R2)
        for part in range(2):

            def norm_rows(i, carry, part=part):
                lo = pl.multiple_of(base + part * R2 + i * 16, 16)
                to = pl.multiple_of(part * R2 + i * 16, 16)
                vals = [
                    x2g[pl.ds(lo, 16), pos * LANES : (pos + 1) * LANES].astype(F32)
                    for pos in range(NTP)
                ]
                total = sum(v * v for v in vals)
                rs = lax.rsqrt(jnp.sum(total, axis=1, keepdims=True) * (1.0 / FULL) + EPS)
                for pos in range(NTP):
                    j = true_block(part, pos)
                    nrm[pl.ds(to, 16), j * LANES : (j + 1) * LANES] = (
                        vals[pos] * rs * gains[1:2, j * LANES : (j + 1) * LANES]
                    ).astype(BF16)
                return carry

            lax.fori_loop(0, R2 // 16, norm_rows, 0)
        hg = jnp.dot(nrm[...], gw[...], preferred_element_type=F32)
        hu = jnp.dot(nrm[...], uw[...], preferred_element_type=F32)
        hid[...] = ((hg / (1.0 + jnp.exp(-hg))) * hu).astype(BF16)
        for q in range(RING):
            p = jnp.dot(
                hid[...], dw[:, q * WIDE : (q + 1) * WIDE], preferred_element_type=F32
            ).astype(BF16)
            part_sum[pl.ds(base, R2), q * WIDE : (q + 1) * WIDE] = p[:R2, :]
            for i in range(RING):
                at = (i * RING + q) * LANES
                part_sum[pl.ds(base + R2, R2), at : at + LANES] = p[
                    R2:, i * LANES : (i + 1) * LANES
                ]
        for part in range(2):
            _, major, _, wide, _, r = ring(part, g, R2, first2)
            push(g, exchange(g, part, 6, part_sum.at[r, wide(2)], t1.at[r], major(1)))
            push(g, exchange(g, part, 7, part_sum.at[r, wide(-1)], v1.at[r], major(-1)))

    def c5(g):
        for part in range(2):
            _, major, _, wide, _, r = ring(part, g, R2, first2)
            exchange(g, part, 6, t1.at[r], t1.at[r], major(1)).wait_recv()
            s1[r, :] = (t1[r, :].astype(F32) + part_sum[r, wide(1)].astype(F32)).astype(BF16)
            push(g, exchange(g, part, 8, s1.at[r], u1.at[r], major(1)))

    def c6(g):
        for part in range(2):
            minor, major, _, wide, small, r = ring(part, g, R2, first2)
            exchange(g, part, 7, v1.at[r], v1.at[r], major(1)).wait_recv()
            exchange(g, part, 8, u1.at[r], u1.at[r], major(1)).wait_recv()
            q1[r, :] = (
                part_sum[r, wide(0)].astype(F32) + u1[r, :].astype(F32) + v1[r, :].astype(F32)
            ).astype(BF16)
            push(g, exchange(g, part, 9, q1.at[r, small(2)], t2.at[r], minor(1)))
            push(g, exchange(g, part, 10, q1.at[r, small(-1)], v2.at[r], minor(-1)))

    def c7(g):
        for part in range(2):
            minor, _, _, _, small, r = ring(part, g, R2, first2)
            exchange(g, part, 9, t2.at[r], t2.at[r], minor(1)).wait_recv()
            s2[r, :] = (t2[r, :].astype(F32) + q1[r, small(1)].astype(F32)).astype(BF16)
            push(g, exchange(g, part, 11, s2.at[r], u2.at[r], minor(1)))

    def back(r):
        dz = distance(r // 2)
        zt = lax.rem(z + dz, NZ)
        ct = lax.rem(c + r, 2)
        lo = pl.multiple_of(r * CAP, CAP)
        return remote(
            fin.at[pl.ds(lo, CAP), :], ret.at[me_sp], rsend, rrecv, (zt, ct, y, x)
        )

    def c8(g):
        for part in range(2):
            minor, _, _, _, small, r = ring(part, g, R2, first2)
            exchange(g, part, 10, v2.at[r], v2.at[r], minor(1)).wait_recv()
            exchange(g, part, 11, u2.at[r], u2.at[r], minor(1)).wait_recv()
            fin[r, :] = (
                q1[r, small(0)].astype(F32) + u2[r, :].astype(F32) + v2[r, :].astype(F32)
            ).astype(BF16)
            for i in range(CHUNKS):
                k = (g * 2 + part) * CHUNKS + i

                @pl.when(k != r_self)
                def _(k=k):
                    back(k).start()

    pipeline(
        (
            (8, c8),
            (7, c7),
            (6, c6),
            (5, c5),
            (3, b3),
            (2, b2),
            (1, b1),
            (0, first_stage),
            (4, expert_stage),
        ),
        G2,
    )
    ret[me_sp] = fin[r_self * CAP : (r_self + 1) * CAP, :]

    bdrain()
    for part in range(2):
        minor, major, _, wide, small, r = ring(part, 0, R2, first2)
        for kind in (6, 7, 8):
            exchange(0, part, kind, t1.at[r], t1.at[r], major(1)).wait_send()
        for kind in (9, 10, 11):
            exchange(0, part, kind, t2.at[r], t2.at[r], minor(1)).wait_send()
    others = ret.at[pl.ds(0, EXPERTS - 1)]
    pltpu.make_async_copy(others, others, dsend).wait()
    pltpu.make_async_copy(others, others, rrecv).wait()
    pltpu.make_async_copy(others, others, rsend).wait()

    back_rows = ret[...].reshape(SLOTS, LANES)
    total = jnp.zeros((ROWS, LANES), F32)
    for k in range(2):
        picked = jnp.dot(pick[k], back_rows, preferred_element_type=F32)
        total = total + picked * to_column(rw[k : k + 1, :])
    out[...] = (strm[...].astype(F32) + total).astype(BF16)


def per_device(
    residual_in,
    conv_value,
    conv_gate,
    doc_ids,
    conv_kernel,
    ln_gain,
    out_weight,
    norm_gain,
    routes,
    route_weight,
    gate_w,
    up_w,
    down_w,
):
    vmem = pl.BlockSpec(memory_space=pltpu.VMEM)
    hbm = pl.BlockSpec(memory_space=pl.ANY)
    dma = pltpu.SemaphoreType.DMA
    hidden = gate_w.shape[2]
    return pl.pallas_call(
        kernel,
        out_shape=jax.ShapeDtypeStruct((ROWS, LANES), BF16),
        in_specs=[vmem] * 9 + [hbm] * 4,
        out_specs=vmem,
        scratch_shapes=[
            pltpu.VMEM((FULL, LANES), BF16),
            pltpu.VMEM((FULL, hidden), BF16),
            pltpu.VMEM((FULL, hidden), BF16),
            pltpu.VMEM((hidden, FULL), BF16),
            pltpu.VMEM((HALO + ROWS, LANES), F32),
            pltpu.VMEM((HALO + ROWS, LANES), F32),
            pltpu.VMEM((HALO, LANES), BF16),
            pltpu.VMEM((HALO, LANES), F32),
            pltpu.VMEM((HALO, LANES), BF16),
            pltpu.VMEM((HALO, LANES), F32),
            pltpu.VMEM((ROWS, LANES), F32),
            pltpu.VMEM((NTP, 8, ROWS), F32),
            pltpu.VMEM((8, FULL), F32),
            pltpu.VMEM((ROWS, LANES), F32),
            pltpu.VMEM((ROWS, FULL), BF16),
            pltpu.VMEM((ROWS, FULL), BF16),
            pltpu.VMEM((ROWS, LANES), BF16),
            pltpu.VMEM((2, ROWS, SLOTS), BF16),
            pltpu.VMEM((EXPERTS, CAP, LANES), BF16),
            pltpu.VMEM((SLOTS, FULL), BF16),
            pltpu.VMEM((2 * R2, FULL), BF16),
            pltpu.VMEM((2 * R2, hidden), BF16),
            pltpu.VMEM((SLOTS, FULL), BF16),
            pltpu.VMEM((SLOTS, WIDE), BF16),
            pltpu.VMEM((SLOTS, WIDE), BF16),
            pltpu.VMEM((SLOTS, WIDE), BF16),
            pltpu.VMEM((SLOTS, WIDE), BF16),
            pltpu.VMEM((SLOTS, WIDE), BF16),
            pltpu.VMEM((SLOTS, LANES), BF16),
            pltpu.VMEM((SLOTS, LANES), BF16),
            pltpu.VMEM((SLOTS, LANES), BF16),
            pltpu.VMEM((SLOTS, LANES), BF16),
            pltpu.VMEM((SLOTS, LANES), BF16),
            pltpu.VMEM((EXPERTS, CAP, LANES), BF16),
            dma((4,)),
            dma((2,)),
            dma((2,)),
            dma((NTP,)),
            dma((NTP,)),
            dma((2, 6)),
            dma((G1, 2, 6)),
            dma((2, 12)),
            dma((G2, 2, 12)),
            dma(()),
            dma((2 * G2,)),
            dma(()),
            dma(()),
        ],
        compiler_params=pltpu.CompilerParams(
            collective_id=0, has_side_effects=True, vmem_limit_bytes=60 * 1024 * 1024
        ),
        name="layer",
    )(
        conv_value,
        conv_gate,
        doc_ids.reshape(1, ROWS),
        conv_kernel,
        ln_gain.reshape(1, LANES),
        residual_in,
        routes.T,
        route_weight.T,
        norm_gain.reshape(1, LANES),
        out_weight,
        gate_w,
        up_w,
        down_w,
    )


def solution(mesh):
    split = Mesh(mesh.devices.reshape(NZ, 2, RING, RING), AXES)
    in_specs = (
        P(SP, TP),
        P(SP, TP),
        P(SP, TP),
        P(SP),
        P(None, TP),
        P(TP),
        P(None, TP),
        P(TP),
        P(SP, None),
        P(SP, None),
        P(SP, None, TP),
        P(SP, None, TP),
        P(SP, TP, None),
    )
    return jax.shard_map(
        per_device, mesh=split, in_specs=in_specs, out_specs=P(SP, TP), check_vma=False
    )
```

```python
import functools

import jax
import jax.numpy as jnp
from jax import lax
from jax.experimental import pallas as pl
from jax.experimental.pallas import tpu as pltpu
from jax.sharding import Mesh
from jax.sharding import PartitionSpec as P

MESH = pl.DeviceIdType.MESH
F32 = jnp.float32
BF16 = jnp.bfloat16
AXES = ("z", "core", "y", "x")
TP = ("y", "x")
SP = ("z", "core")
EPS = 1e-06

ROWS = 256
LANES = 128
RING = 4
NTP = RING * RING
WIDE = RING * LANES
FULL = NTP * LANES
TAPS = 31
HALO = 32
EXPERTS = 32
CAP = 32
SLOTS = EXPERTS * CAP
NZ = 16
G1 = 2
G2 = 4
R1 = ROWS // G1 // 2
R2 = SLOTS // G2 // 2
CHUNKS = R2 // CAP
REACH = (0, 1, 15, 2, 12, 5, 11, 6, 10, 7, 9, 8, 14, 3, 13, 4)
ORDER = (
    0, 1, 10, 11, 20, 21, 100, 101, 30, 31, 110, 111,
    120, 121, 201, 200, 131, 130, 210, 211, 221, 220, 300, 230,
    231, 310, 320, 400, 401, 330, 410, 411, 420, 421, 500, 501,
    430, 431, 510, 511, 520, 521, 600, 601, 530, 531, 610, 611,
    620, 621, 630, 631,
)


def remote(src, dst, send, recv, dev):
    return pltpu.make_async_remote_copy(
        src_ref=src,
        dst_ref=dst,
        send_sem=send,
        recv_sem=recv,
        device_id=dev,
        device_id_type=MESH,
    )


def to_column(row):
    return jnp.transpose(jnp.broadcast_to(row, (LANES, row.shape[1])))


def true_block(part, pos):
    return pos if part == 0 else (pos % RING) * RING + pos // RING


def kernel(
    cv,
    cg,
    doc,
    ck,
    lng,
    res,
    routes,
    rw,
    ng,
    ow_hbm,
    gw_hbm,
    uw_hbm,
    dw_hbm,
    out,
    ow,
    gw,
    uw,
    dw,
    ext,
    docx,
    hg_out,
    hd_out,
    hg_in,
    hd_in,
    conv,
    stat,
    gains,
    colstat,
    xg,
    act,
    strm,
    pick,
    dsp,
    x2g,
    nrm,
    hid,
    part_sum,
    t1,
    u1,
    v1,
    s1,
    q1,
    t2,
    u2,
    v2,
    s2,
    fin,
    ret,
    wsem,
    hsend,
    hrecv,
    stsend,
    strecv,
    ssem1,
    rsem1,
    ssem2,
    rsem2,
    dsend,
    drecv,
    rsend,
    rrecv,
    ready,
):
    z = lax.axis_index("z")
    c = lax.axis_index("core")
    y = lax.axis_index("y")
    x = lax.axis_index("x")
    me_tp = y * RING + x
    me_sp = z * 2 + c

    weights = [
        pltpu.make_async_copy(src, dst, wsem.at[i])
        for i, (src, dst) in enumerate(
            ((ow_hbm, ow), (gw_hbm.at[0], gw), (uw_hbm.at[0], uw), (dw_hbm.at[0], dw))
        )
    ]
    for w in weights:
        w.start()

    barrier = pltpu.get_barrier_semaphore()

    def tp_peer(k):
        other = lax.rem(me_tp + k, NTP)
        return (z, c, other // RING, lax.rem(other, RING))

    def along(by, core):
        return (lax.rem(z + by + NZ, NZ), core, y, x)

    def tell(sem, dev):
        pl.semaphore_signal(sem, inc=1, device_id=dev, device_id_type=MESH)

    def greet(k, carry):
        tell(barrier, tp_peer(k))
        return carry

    beside = along(2 * c - 1, 1 - c)
    for dev in (along(1, c), along(-1, c), along(0, 1 - c), beside):
        tell(barrier, dev)
    lax.fori_loop(1, NTP, greet, 0)

    gate = cg[...].astype(F32)
    gated = (cv[...].astype(F32) * (1.0 / (1.0 + jnp.exp(-gate)))).astype(BF16)
    ext[HALO:, :] = gated.astype(F32)
    hg_out[...] = gated[ROWS - HALO :, :]
    dcol = to_column(doc[...].astype(F32))
    docx[HALO:, :] = dcol
    hd_out[...] = dcol[ROWS - HALO :, :]
    taps = ck[...].astype(F32)

    def conv_rows(first, count):
        acc = jnp.zeros((count, LANES), F32)
        mine = docx[HALO + first : HALO + first + count, :]
        for tap in range(TAPS):
            at = HALO + first - (TAPS - 1) + tap
            same = docx[at : at + count, :] == mine
            term = ext[at : at + count, :] * taps[tap : tap + 1, :]
            acc = acc + jnp.where(same, term, 0.0)
        conv[first : first + count, :] = acc

    for first in range(HALO, ROWS, 32):
        conv_rows(first, 32)

    pl.semaphore_wait(barrier, NTP - 1 + 4)

    def spread_word(i):
        if i > 0:
            pl.semaphore_wait(ready.at[i - 1], 1 if i == 1 else 2)
        if i == 0:
            tell(ready.at[0], along(0, 1 - c))
        elif i < 4:
            for by in (1 << (i - 1), -(1 << (i - 1))):
                tell(ready.at[i], along(by, c))

    spread_word(0)
    after = along(c, 1 - c)
    halo_g = remote(hg_out, hg_in, hsend.at[0], hrecv.at[0], after)
    halo_d = remote(hd_out, hd_in, hsend.at[1], hrecv.at[1], after)
    halo_g.start()
    halo_d.start()

    ids = routes[...]
    expert = lax.broadcasted_iota(jnp.int32, (EXPERTS, ROWS), 0)
    names = [(expert == ids[k : k + 1, :]).astype(F32) for k in range(2)]
    before = (
        lax.broadcasted_iota(jnp.int32, (ROWS, ROWS), 0)
        < lax.broadcasted_iota(jnp.int32, (ROWS, ROWS), 1)
    ).astype(F32)
    earlier = jnp.dot(
        (names[0] + names[1]).astype(BF16), before.astype(BF16), preferred_element_type=F32
    )
    slot_base = expert.astype(F32) * float(CAP)
    slots = [jnp.sum(n * (earlier + slot_base), axis=0, keepdims=True) for n in names]
    lane = lax.broadcasted_iota(jnp.int32, (ROWS, LANES), 1).astype(F32)
    for k in range(2):
        col = to_column(slots[k])
        for b in range(SLOTS // LANES):
            pick[k, :, b * LANES : (b + 1) * LANES] = (
                (lane + float(b * LANES)) == col
            ).astype(BF16)

    halo_g.wait()
    halo_d.wait()
    spread_word(1)
    first_block = me_sp == 0
    ext[:HALO, :] = hg_in[...].astype(F32)
    docx[:HALO, :] = jnp.where(first_block, -1.0, hd_in[...])
    conv_rows(0, HALO)

    cx = conv[...]
    cxt = jnp.transpose(cx)
    local = jnp.sum(cxt, axis=0, keepdims=True) * (1.0 / LANES)
    spread = cxt - local
    second = jnp.sum(spread * spread, axis=0, keepdims=True)
    gain_row = jnp.concatenate([lng[...].astype(F32), ng[...].astype(F32)], axis=1)
    stat[me_tp] = jnp.concatenate(
        [local, second, gain_row, jnp.zeros((5, ROWS), F32)], axis=0
    )
    dev = (cx - to_column(local)).astype(BF16)
    for g in range(G1):
        for part in range(2):
            mm, mj = (x, y) if part == 0 else (y, x)
            lo = g * 2 * R1 + part * R1
            pos = pl.multiple_of((mj * RING + mm) * LANES, LANES)
            xg[lo : lo + R1, pl.ds(pos, LANES)] = dev[lo : lo + R1, :]

    def send_stat(k, carry):
        remote(stat.at[me_tp], stat.at[me_tp], stsend.at[k], strecv.at[k], tp_peer(k)).start()
        return carry

    def ring(part, g, rows, first):
        mm, mj = (x, y) if part == 0 else (y, x)
        step = 1 - 2 * (g % 2)

        def at(base, by):
            return lax.rem(base + by * step + 2 * RING, RING)

        def minor(by):
            m = at(mm, by)
            return (z, c, mj, m) if part == 0 else (z, c, m, mj)

        def major(by):
            m = at(mj, by)
            return (z, c, m, mm) if part == 0 else (z, c, mm, m)

        def block(by):
            return pl.ds(pl.multiple_of((mj * RING + at(mm, by)) * LANES, LANES), LANES)

        def wide(by):
            return pl.ds(pl.multiple_of(at(mj, by) * WIDE, WIDE), WIDE)

        def small(by):
            return pl.ds(pl.multiple_of(at(mm, by) * LANES, LANES), LANES)

        return minor, major, block, wide, small, pl.ds(first(g, part), rows)

    flying = {}

    def push(ssem, part, kind, d):
        key = (id(ssem), part, kind)
        if key in flying:
            flying[key].wait_send()
        d.start()
        flying[key] = d

    def make_gather(buf, rows, first, ssem, rsem):
        def move(g, part, kind, cols, dev):
            ref = buf.at[pl.ds(first(g, part), rows), cols]
            return remote(ref, ref, ssem.at[part, kind], rsem.at[g, part, kind], dev)

        def own(g, part):
            minor, _, block, _, _, _ = ring(part, g, rows, first)
            for kind, by in enumerate((1, -1, 2)):
                push(ssem, part, kind, move(g, part, kind, block(0), minor(by)))

        def sets(g, part):
            minor, major, block, wide, _, _ = ring(part, g, rows, first)
            for kind, by in enumerate((-1, 1, 2)):
                move(g, part, kind, block(by), minor(1)).wait_recv()
            push(ssem, part, 3, move(g, part, 3, wide(0), major(1)))
            push(ssem, part, 4, move(g, part, 4, wide(0), major(-1)))

        def relay(g, part):
            _, major, _, wide, _, _ = ring(part, g, rows, first)
            move(g, part, 3, wide(-1), major(1)).wait_recv()
            push(ssem, part, 5, move(g, part, 5, wide(-1), major(1)))

        def landed(g, part):
            _, major, _, wide, _, _ = ring(part, g, rows, first)
            move(g, part, 4, wide(1), major(1)).wait_recv()
            move(g, part, 5, wide(2), major(1)).wait_recv()

        return own, sets, relay, landed

    def first1(g, part):
        return g * 2 * R1 + part * R1

    own1, sets1, relay1, landed1 = make_gather(xg, R1, first1, ssem1, rsem1)
    moves1 = [(g, part) for g in range(G1) for part in range(2)]
    for g, part in moves1:
        own1(g, part)
    lax.fori_loop(1, NTP, send_stat, 0)
    spread_word(2)
    for g, part in moves1:
        sets1(g, part)
    spread_word(3)

    def wait_stat(k, carry):
        d = remote(stat.at[me_tp], stat.at[me_tp], stsend.at[k], strecv.at[k], tp_peer(k))
        d.wait_send()
        d.wait_recv()
        return carry

    lax.fori_loop(1, NTP, wait_stat, 0)
    for g, part in moves1[:2]:
        relay1(g, part)

    means = [stat[j, 0:1, :] for j in range(NTP)]
    mean = sum(means) * (1.0 / NTP)
    shifts = [m - mean for m in means]
    var = (
        sum(stat[j, 1:2, :] for j in range(NTP)) * (1.0 / FULL)
        + sum(s * s for s in shifts) * (1.0 / NTP)
    )
    scale = lax.rsqrt(var + EPS)
    table = jnp.concatenate(shifts + [scale] + [jnp.zeros((LANES - NTP - 1, ROWS), F32)], axis=0)
    colstat[...] = jnp.transpose(table)
    for j in range(NTP):
        gains[:, j * LANES : (j + 1) * LANES] = jnp.concatenate(
            [stat[j, 2:3, :LANES], stat[j, 2:3, LANES:], jnp.zeros((6, LANES), F32)], axis=0
        )

    def normalise(g, part):
        landed1(g, part)

        def some(i, carry):
            lo = pl.multiple_of(first1(g, part) + i * 16, 16)
            cs = colstat[pl.ds(lo, 16), :]
            rs = cs[:, NTP : NTP + 1]
            for pos in range(NTP):
                j = true_block(part, pos)
                v = xg[pl.ds(lo, 16), pos * LANES : (pos + 1) * LANES].astype(F32)
                v = (v + cs[:, j : j + 1]) * rs * gains[0:1, j * LANES : (j + 1) * LANES]
                v = v / (1.0 + jnp.exp(-v))
                act[pl.ds(lo, 16), j * LANES : (j + 1) * LANES] = v.astype(BF16)
            return carry

        lax.fori_loop(0, R1 // 16, some, 0)

    for i, (g, part) in enumerate(moves1):
        if i + 2 < len(moves1):
            relay1(*moves1[i + 2])
        normalise(g, part)
    spread_word(4)

    weights[0].wait()
    projected = jnp.dot(act[...], ow[...], preferred_element_type=F32).astype(BF16)
    strm[...] = (res[...].astype(F32) + projected.astype(F32)).astype(BF16)

    slot = lax.broadcasted_iota(jnp.int32, (SLOTS, ROWS), 0).astype(F32)
    chosen = ((slot == slots[0]) | (slot == slots[1])).astype(BF16)
    dsp[...] = (
        jnp.dot(chosen, strm[...], preferred_element_type=F32)
        .astype(BF16)
        .reshape(EXPERTS, CAP, LANES)
    )

    own_pos = [
        pl.multiple_of((y * RING + x) * LANES, LANES),
        pl.multiple_of((x * RING + y) * LANES, LANES),
    ]

    def here(r):
        part = (r // CHUNKS) % 2
        return x2g.at[pl.ds(r * CAP, CAP), pl.ds(own_pos[part], LANES)]

    for r in range(1, EXPERTS):
        dev = along(-REACH[r // 2], lax.rem(c + r, 2))
        remote(dsp.at[dev[0] * 2 + dev[1]], here(r), dsend, drecv.at[r // CHUNKS], dev).start()
    x2g[:CAP, pl.ds(own_pos[0], LANES)] = dsp[me_sp]

    def first2(g, part):
        return g * 2 * R2 + part * R2

    own2, sets2, relay2, landed2 = make_gather(x2g, R2, first2, ssem2, rsem2)

    def arrived(g, part):
        rows = R2 - CAP if g + part == 0 else R2
        ref = x2g.at[pl.ds(first2(g, part), rows), pl.ds(own_pos[part], LANES)]
        pltpu.make_async_copy(ref, ref, drecv.at[g * 2 + part]).wait()
        own2(g, part)

    for w in weights[1:]:
        w.wait()

    def exchange(g, part, kind, src, dst, dev):
        return remote(src, dst, ssem2.at[part, kind], rsem2.at[g, part, kind], dev)

    def expert_stage(g, _):
        landed2(g, 0)
        landed2(g, 1)
        base = g * 2 * R2
        for part in range(2):

            def norm_rows(i, carry, part=part):
                lo = pl.multiple_of(base + part * R2 + i * 16, 16)
                to = pl.multiple_of(part * R2 + i * 16, 16)
                vals = [
                    x2g[pl.ds(lo, 16), pos * LANES : (pos + 1) * LANES].astype(F32)
                    for pos in range(NTP)
                ]
                total = sum(v * v for v in vals)
                rs = lax.rsqrt(jnp.sum(total, axis=1, keepdims=True) * (1.0 / FULL) + EPS)
                for pos in range(NTP):
                    j = true_block(part, pos)
                    nrm[pl.ds(to, 16), j * LANES : (j + 1) * LANES] = (
                        vals[pos] * rs * gains[1:2, j * LANES : (j + 1) * LANES]
                    ).astype(BF16)
                return carry

            lax.fori_loop(0, R2 // 16, norm_rows, 0)
        hg = jnp.dot(nrm[...], gw[...], preferred_element_type=F32)
        hu = jnp.dot(nrm[...], uw[...], preferred_element_type=F32)
        hid[...] = ((hg / (1.0 + jnp.exp(-hg))) * hu).astype(BF16)
        for q in range(RING):
            p = jnp.dot(
                hid[...], dw[:, q * WIDE : (q + 1) * WIDE], preferred_element_type=F32
            ).astype(BF16)
            part_sum[pl.ds(base, R2), q * WIDE : (q + 1) * WIDE] = p[:R2, :]
            for i in range(RING):
                at = (i * RING + q) * LANES
                part_sum[pl.ds(base + R2, R2), at : at + LANES] = p[
                    R2:, i * LANES : (i + 1) * LANES
                ]
        for part in range(2):
            _, major, _, wide, _, r = ring(part, g, R2, first2)
            send(g, part, 6, part_sum.at[r, wide(2)], t1.at[r], major(1))
            send(g, part, 7, part_sum.at[r, wide(-1)], v1.at[r], major(-1))

    def send(g, part, kind, src, dst, dev):
        push(ssem2, part, kind, exchange(g, part, kind, src, dst, dev))

    def pass_on(g, part):
        _, major, _, wide, _, r = ring(part, g, R2, first2)
        exchange(g, part, 6, t1.at[r], t1.at[r], major(1)).wait_recv()
        s1[r, :] = (t1[r, :].astype(F32) + part_sum[r, wide(1)].astype(F32)).astype(BF16)
        send(g, part, 8, s1.at[r], u1.at[r], major(1))

    def ring_sum(g, part):
        minor, major, _, wide, small, r = ring(part, g, R2, first2)
        exchange(g, part, 7, v1.at[r], v1.at[r], major(1)).wait_recv()
        exchange(g, part, 8, u1.at[r], u1.at[r], major(1)).wait_recv()
        q1[r, :] = (
            part_sum[r, wide(0)].astype(F32) + u1[r, :].astype(F32) + v1[r, :].astype(F32)
        ).astype(BF16)
        for kind, by, dst in ((9, 1, t2), (10, -1, v2), (11, 2, u2)):
            send(g, part, kind, q1.at[r, small(by)], dst.at[r], minor(by))

    def last_sum(g, part):
        minor, _, _, _, small, r = ring(part, g, R2, first2)
        total = q1[r, small(0)].astype(F32)
        for kind, dst in ((9, t2), (10, v2), (11, u2)):
            exchange(g, part, kind, dst.at[r], dst.at[r], minor(1)).wait_recv()
        fin[r, :] = (
            total + t2[r, :].astype(F32) + v2[r, :].astype(F32) + u2[r, :].astype(F32)
        ).astype(BF16)
        for i in range(CHUNKS):
            k = (g * 2 + part) * CHUNKS + i
            if k > 0:
                dev = along(REACH[k // 2], lax.rem(c + k, 2))
                src = fin.at[pl.ds(k * CAP, CAP), :]
                remote(src, ret.at[me_sp], rsend, rrecv, dev).start()

    moves2 = (arrived, sets2, relay2, expert_stage, pass_on, ring_sum, last_sum)
    for code in ORDER:
        moves2[code // 100](code // 10 % 10, code % 10)
    ret[me_sp] = fin[:CAP, :]

    for d in flying.values():
        d.wait_send()
    others = ret.at[pl.ds(0, EXPERTS - 1)]
    pltpu.make_async_copy(others, others, dsend).wait()
    pltpu.make_async_copy(others, others, rrecv).wait()
    pltpu.make_async_copy(others, others, rsend).wait()

    back_rows = ret[...].reshape(SLOTS, LANES)
    total = jnp.zeros((ROWS, LANES), F32)
    for k in range(2):
        picked = jnp.dot(pick[k], back_rows, preferred_element_type=F32)
        total = total + picked * to_column(rw[k : k + 1, :])
    out[...] = (strm[...].astype(F32) + total).astype(BF16)


def per_device(
    residual_in,
    conv_value,
    conv_gate,
    doc_ids,
    conv_kernel,
    ln_gain,
    out_weight,
    norm_gain,
    routes,
    route_weight,
    gate_w,
    up_w,
    down_w,
):
    vmem = pl.BlockSpec(memory_space=pltpu.VMEM)
    hbm = pl.BlockSpec(memory_space=pl.ANY)
    dma = pltpu.SemaphoreType.DMA
    hidden = gate_w.shape[2]
    return pl.pallas_call(
        kernel,
        out_shape=jax.ShapeDtypeStruct((ROWS, LANES), BF16),
        in_specs=[vmem] * 9 + [hbm] * 4,
        out_specs=vmem,
        scratch_shapes=[
            pltpu.VMEM((FULL, LANES), BF16),
            pltpu.VMEM((FULL, hidden), BF16),
            pltpu.VMEM((FULL, hidden), BF16),
            pltpu.VMEM((hidden, FULL), BF16),
            pltpu.VMEM((HALO + ROWS, LANES), F32),
            pltpu.VMEM((HALO + ROWS, LANES), F32),
            pltpu.VMEM((HALO, LANES), BF16),
            pltpu.VMEM((HALO, LANES), F32),
            pltpu.VMEM((HALO, LANES), BF16),
            pltpu.VMEM((HALO, LANES), F32),
            pltpu.VMEM((ROWS, LANES), F32),
            pltpu.VMEM((NTP, 8, ROWS), F32),
            pltpu.VMEM((8, FULL), F32),
            pltpu.VMEM((ROWS, LANES), F32),
            pltpu.VMEM((ROWS, FULL), BF16),
            pltpu.VMEM((ROWS, FULL), BF16),
            pltpu.VMEM((ROWS, LANES), BF16),
            pltpu.VMEM((2, ROWS, SLOTS), BF16),
            pltpu.VMEM((EXPERTS, CAP, LANES), BF16),
            pltpu.VMEM((SLOTS, FULL), BF16),
            pltpu.VMEM((2 * R2, FULL), BF16),
            pltpu.VMEM((2 * R2, hidden), BF16),
            pltpu.VMEM((SLOTS, FULL), BF16),
            pltpu.VMEM((SLOTS, WIDE), BF16),
            pltpu.VMEM((SLOTS, WIDE), BF16),
            pltpu.VMEM((SLOTS, WIDE), BF16),
            pltpu.VMEM((SLOTS, WIDE), BF16),
            pltpu.VMEM((SLOTS, WIDE), BF16),
            pltpu.VMEM((SLOTS, LANES), BF16),
            pltpu.VMEM((SLOTS, LANES), BF16),
            pltpu.VMEM((SLOTS, LANES), BF16),
            pltpu.VMEM((SLOTS, LANES), BF16),
            pltpu.VMEM((SLOTS, LANES), BF16),
            pltpu.VMEM((EXPERTS, CAP, LANES), BF16),
            dma((4,)),
            dma((2,)),
            dma((2,)),
            dma((NTP,)),
            dma((NTP,)),
            dma((2, 6)),
            dma((G1, 2, 6)),
            dma((2, 12)),
            dma((G2, 2, 12)),
            dma(()),
            dma((2 * G2,)),
            dma(()),
            dma(()),
            pltpu.SemaphoreType.REGULAR((4,)),
        ],
        compiler_params=pltpu.CompilerParams(
            collective_id=0, has_side_effects=True, vmem_limit_bytes=60 * 1024 * 1024
        ),
        name="layer",
    )(
        conv_value,
        conv_gate,
        doc_ids.reshape(1, ROWS),
        conv_kernel,
        ln_gain.reshape(1, LANES),
        residual_in,
        routes.T,
        route_weight.T,
        norm_gain.reshape(1, LANES),
        out_weight,
        gate_w,
        up_w,
        down_w,
    )


def solution(mesh):
    split = Mesh(mesh.devices.reshape(NZ, 2, RING, RING), AXES)
    in_specs = (
        P(SP, TP),
        P(SP, TP),
        P(SP, TP),
        P(SP),
        P(None, TP),
        P(TP),
        P(None, TP),
        P(TP),
        P(SP, None),
        P(SP, None),
        P(SP, None, TP),
        P(SP, None, TP),
        P(SP, TP, None),
    )
    return jax.shard_map(
        per_device, mesh=split, in_specs=in_specs, out_specs=P(SP, TP), check_vma=False
    )
```

```python
import functools

import jax
import jax.numpy as jnp
from jax import lax
from jax.experimental import pallas as pl
from jax.experimental.pallas import tpu as pltpu
from jax.sharding import Mesh
from jax.sharding import PartitionSpec as P

MESH = pl.DeviceIdType.MESH
F32 = jnp.float32
BF16 = jnp.bfloat16
AXES = ("z", "core", "y", "x")
TP = ("y", "x")
SP = ("z", "core")
EPS = 1e-06

ROWS = 256
LANES = 128
RING = 4
NTP = RING * RING
WIDE = RING * LANES
FULL = NTP * LANES
TAPS = 31
HALO = 32
EXPERTS = 32
CAP = 32
SLOTS = EXPERTS * CAP
NZ = 16
G1 = 2
R1 = ROWS // G1 // 2
SIZES = (2, 4, 4, 4, 2)
G2 = len(SIZES)
BIG = 2 * max(SIZES) * CAP
REACH = (0, 1, 15, 2, 12, 5, 11, 6, 10, 7, 9, 8, 14, 3, 13, 4)
ORDER = (
    0, 1, 10, 11, 100, 101, 20, 21, 110, 111, 200, 201,
    30, 31, 120, 121, 210, 211, 300, 40, 41, 130, 131, 220,
    221, 310, 140, 141, 230, 231, 400, 401, 320, 240, 241, 410,
    411, 330, 500, 501, 420, 421, 340, 510, 511, 600, 601, 430,
    431, 520, 521, 610, 611, 440, 441, 530, 531, 620, 621, 540,
    541, 630, 631, 640, 641,
)


def remote(src, dst, send, recv, dev):
    return pltpu.make_async_remote_copy(
        src_ref=src,
        dst_ref=dst,
        send_sem=send,
        recv_sem=recv,
        device_id=dev,
        device_id_type=MESH,
    )


def to_column(row):
    return jnp.transpose(jnp.broadcast_to(row, (LANES, row.shape[1])))


def first_chunk(g, part):
    return 2 * sum(SIZES[:g]) + part * SIZES[g]


def first2(g, part):
    return first_chunk(g, part) * CAP


def rows2(g):
    return SIZES[g] * CAP


def rows1(g):
    return R1


PLACE = [(g, p) for g in range(G2) for p in range(2) for _ in range(SIZES[g])]


def true_block(part, pos):
    return pos if part == 0 else (pos % RING) * RING + pos // RING


def kernel(
    cv_hbm,
    cg_hbm,
    doc_hbm,
    ck_hbm,
    lng_hbm,
    res_hbm,
    routes_hbm,
    rw_hbm,
    ng_hbm,
    ow_hbm,
    gw_hbm,
    uw_hbm,
    dw_hbm,
    out,
    ow,
    gw,
    uw,
    dw,
    ext,
    docx,
    hg_out,
    hd_out,
    hg_in,
    hd_in,
    conv,
    stat,
    gains,
    colstat,
    xg,
    act,
    strm,
    pick,
    dsp,
    x2g,
    nrm,
    hid,
    part_sum,
    t1,
    u1,
    v1,
    s1,
    q1,
    t2,
    u2,
    v2,
    s2,
    fin,
    ret,
    wsem,
    hsend,
    hrecv,
    stsend,
    strecv,
    ssem1,
    rsem1,
    ssem2,
    rsem2,
    dsend,
    drecv,
    rsend,
    rrecv,
    ready,
    cv,
    cg,
    doc,
    ck,
    lng,
    res,
    routes,
    rw,
    ng,
    isem,
):
    z = lax.axis_index("z")
    c = lax.axis_index("core")
    y = lax.axis_index("y")
    x = lax.axis_index("x")
    me_tp = y * RING + x
    me_sp = z * 2 + c

    weights = [
        pltpu.make_async_copy(src, dst, wsem.at[i])
        for i, (src, dst) in enumerate(
            ((ow_hbm, ow), (gw_hbm.at[0], gw), (uw_hbm.at[0], uw), (dw_hbm.at[0], dw))
        )
    ]
    small_inputs = [
        pltpu.make_async_copy(src, dst, isem.at[i])
        for i, (src, dst) in enumerate(
            zip(
                (cv_hbm, cg_hbm, doc_hbm, ck_hbm, routes_hbm, lng_hbm, ng_hbm, rw_hbm, res_hbm),
                (cv, cg, doc, ck, routes, lng, ng, rw, res),
            )
        )
    ]
    for w in small_inputs:
        w.start()

    barrier = pltpu.get_barrier_semaphore()

    def tp_peer(k):
        other = lax.rem(me_tp + k, NTP)
        return (z, c, other // RING, lax.rem(other, RING))

    def along(by, core):
        return (lax.rem(z + by + NZ, NZ), core, y, x)

    def tell(sem, dev):
        pl.semaphore_signal(sem, inc=1, device_id=dev, device_id_type=MESH)

    def greet(k, carry):
        tell(barrier, tp_peer(k))
        return carry

    beside = along(2 * c - 1, 1 - c)
    for dev in (along(1, c), along(-1, c), along(0, 1 - c), beside):
        tell(barrier, dev)
    lax.fori_loop(1, NTP, greet, 0)

    for w in weights:
        w.start()
    for w in small_inputs:
        w.wait()

    gate = cg[...].astype(F32)
    gated = (cv[...].astype(F32) * (1.0 / (1.0 + jnp.exp(-gate)))).astype(BF16)
    ext[HALO:, :] = gated.astype(F32)
    hg_out[...] = gated[ROWS - HALO :, :]
    dcol = to_column(doc[...].astype(F32))
    docx[HALO:, :] = dcol
    hd_out[...] = dcol[ROWS - HALO :, :]
    taps = ck[...].astype(F32)

    def conv_rows(first, count):
        acc = jnp.zeros((count, LANES), F32)
        mine = docx[HALO + first : HALO + first + count, :]
        for tap in range(TAPS):
            at = HALO + first - (TAPS - 1) + tap
            same = docx[at : at + count, :] == mine
            term = ext[at : at + count, :] * taps[tap : tap + 1, :]
            acc = acc + jnp.where(same, term, 0.0)
        conv[first : first + count, :] = acc

    for first in range(HALO, ROWS, 32):
        conv_rows(first, 32)

    pl.semaphore_wait(barrier, NTP - 1 + 4)

    def spread_word(i):
        if i > 0:
            pl.semaphore_wait(ready.at[i - 1], 1 if i == 1 else 2)
        if i == 0:
            tell(ready.at[0], along(0, 1 - c))
        elif i < 4:
            for by in (1 << (i - 1), -(1 << (i - 1))):
                tell(ready.at[i], along(by, c))

    spread_word(0)
    after = along(c, 1 - c)
    halo_g = remote(hg_out, hg_in, hsend.at[0], hrecv.at[0], after)
    halo_d = remote(hd_out, hd_in, hsend.at[1], hrecv.at[1], after)

    @pl.when(me_sp < 2 * NZ - 1)
    def _():
        halo_g.start()
        halo_d.start()

    ids = routes[...]
    expert = lax.broadcasted_iota(jnp.int32, (EXPERTS, ROWS), 0)
    names = [(expert == ids[k : k + 1, :]).astype(F32) for k in range(2)]
    before = (
        lax.broadcasted_iota(jnp.int32, (ROWS, ROWS), 0)
        < lax.broadcasted_iota(jnp.int32, (ROWS, ROWS), 1)
    ).astype(F32)
    earlier = jnp.dot(
        (names[0] + names[1]).astype(BF16), before.astype(BF16), preferred_element_type=F32
    )
    slot_base = expert.astype(F32) * float(CAP)
    slots = [jnp.sum(n * (earlier + slot_base), axis=0, keepdims=True) for n in names]
    lane = lax.broadcasted_iota(jnp.int32, (ROWS, LANES), 1).astype(F32)
    for k in range(2):
        col = to_column(slots[k])
        for b in range(SLOTS // LANES):
            pick[k, :, b * LANES : (b + 1) * LANES] = (
                (lane + float(b * LANES)) == col
            ).astype(BF16)

    first_block = me_sp == 0

    @pl.when(me_sp > 0)
    def _():
        halo_g.wait_recv()
        halo_d.wait_recv()

    spread_word(1)
    ext[:HALO, :] = jnp.where(first_block, 0.0, hg_in[...].astype(F32))
    docx[:HALO, :] = jnp.where(first_block, -1.0, hd_in[...])
    conv_rows(0, HALO)

    cx = conv[...]
    cxt = jnp.transpose(cx)
    local = jnp.sum(cxt, axis=0, keepdims=True) * (1.0 / LANES)
    spread = cxt - local
    second = jnp.sum(spread * spread, axis=0, keepdims=True)
    gain_row = jnp.concatenate([lng[...].astype(F32), ng[...].astype(F32)], axis=1)
    stat[me_tp] = jnp.concatenate(
        [local, second, gain_row, jnp.zeros((5, ROWS), F32)], axis=0
    )
    dev = (cx - to_column(local)).astype(BF16)
    for g in range(G1):
        for part in range(2):
            mm, mj = (x, y) if part == 0 else (y, x)
            lo = g * 2 * R1 + part * R1
            pos = pl.multiple_of((mj * RING + mm) * LANES, LANES)
            xg[lo : lo + R1, pl.ds(pos, LANES)] = dev[lo : lo + R1, :]

    def send_stat(k, carry):
        remote(stat.at[me_tp], stat.at[me_tp], stsend.at[k], strecv.at[k], tp_peer(k)).start()
        return carry

    def ring(part, g, rows, first):
        mm, mj = (x, y) if part == 0 else (y, x)
        step = 1 - 2 * (g % 2)

        def at(base, by):
            return lax.rem(base + by * step + 2 * RING, RING)

        def minor(by):
            m = at(mm, by)
            return (z, c, mj, m) if part == 0 else (z, c, m, mj)

        def major(by):
            m = at(mj, by)
            return (z, c, m, mm) if part == 0 else (z, c, mm, m)

        def block(by):
            return pl.ds(pl.multiple_of((mj * RING + at(mm, by)) * LANES, LANES), LANES)

        def wide(by):
            return pl.ds(pl.multiple_of(at(mj, by) * WIDE, WIDE), WIDE)

        def small(by):
            return pl.ds(pl.multiple_of(at(mm, by) * LANES, LANES), LANES)

        return minor, major, block, wide, small, pl.ds(first(g, part), rows(g))

    flying = {}

    def push(ssem, part, kind, d):
        key = (id(ssem), part, kind)
        if key in flying:
            flying[key].wait_send()
        d.start()
        flying[key] = d

    def make_gather(buf, rows, first, ssem, rsem):
        def move(g, part, kind, cols, dev):
            ref = buf.at[pl.ds(first(g, part), rows(g)), cols]
            return remote(ref, ref, ssem.at[part, kind], rsem.at[g, part, kind], dev)

        def own(g, part):
            minor, _, block, _, _, _ = ring(part, g, rows, first)
            for kind, by in enumerate((1, -1, 2)):
                push(ssem, part, kind, move(g, part, kind, block(0), minor(by)))

        def sets(g, part):
            minor, major, block, wide, _, _ = ring(part, g, rows, first)
            for kind, by in enumerate((-1, 1, 2)):
                move(g, part, kind, block(by), minor(1)).wait_recv()
            push(ssem, part, 3, move(g, part, 3, wide(0), major(1)))
            push(ssem, part, 4, move(g, part, 4, wide(0), major(-1)))

        def relay(g, part):
            _, major, _, wide, _, _ = ring(part, g, rows, first)
            move(g, part, 3, wide(-1), major(1)).wait_recv()
            push(ssem, part, 5, move(g, part, 5, wide(-1), major(1)))

        def landed(g, part):
            _, major, _, wide, _, _ = ring(part, g, rows, first)
            move(g, part, 4, wide(1), major(1)).wait_recv()
            move(g, part, 5, wide(2), major(1)).wait_recv()

        return own, sets, relay, landed

    def first1(g, part):
        return g * 2 * R1 + part * R1

    own1, sets1, relay1, landed1 = make_gather(xg, rows1, first1, ssem1, rsem1)
    moves1 = [(g, part) for g in range(G1) for part in range(2)]
    for g, part in moves1:
        own1(g, part)
    lax.fori_loop(1, NTP, send_stat, 0)
    spread_word(2)
    for g, part in moves1:
        sets1(g, part)
    spread_word(3)

    def wait_stat(k, carry):
        d = remote(stat.at[me_tp], stat.at[me_tp], stsend.at[k], strecv.at[k], tp_peer(k))
        d.wait_send()
        d.wait_recv()
        return carry

    lax.fori_loop(1, NTP, wait_stat, 0)
    for g, part in moves1[:2]:
        relay1(g, part)

    means = [stat[j, 0:1, :] for j in range(NTP)]
    mean = sum(means) * (1.0 / NTP)
    shifts = [m - mean for m in means]
    var = (
        sum(stat[j, 1:2, :] for j in range(NTP)) * (1.0 / FULL)
        + sum(s * s for s in shifts) * (1.0 / NTP)
    )
    scale = lax.rsqrt(var + EPS)
    table = jnp.concatenate(shifts + [scale] + [jnp.zeros((LANES - NTP - 1, ROWS), F32)], axis=0)
    colstat[...] = jnp.transpose(table)
    for j in range(NTP):
        gains[:, j * LANES : (j + 1) * LANES] = jnp.concatenate(
            [stat[j, 2:3, :LANES], stat[j, 2:3, LANES:], jnp.zeros((6, LANES), F32)], axis=0
        )

    def normalise(g, part):
        landed1(g, part)

        def some(i, carry):
            lo = pl.multiple_of(first1(g, part) + i * 16, 16)
            cs = colstat[pl.ds(lo, 16), :]
            rs = cs[:, NTP : NTP + 1]
            for pos in range(NTP):
                j = true_block(part, pos)
                v = xg[pl.ds(lo, 16), pos * LANES : (pos + 1) * LANES].astype(F32)
                v = (v + cs[:, j : j + 1]) * rs * gains[0:1, j * LANES : (j + 1) * LANES]
                v = v / (1.0 + jnp.exp(-v))
                act[pl.ds(lo, 16), j * LANES : (j + 1) * LANES] = v.astype(BF16)
            return carry

        lax.fori_loop(0, R1 // 16, some, 0)

    for i, (g, part) in enumerate(moves1):
        if i + 2 < len(moves1):
            relay1(*moves1[i + 2])
        normalise(g, part)
    spread_word(4)

    weights[0].wait()
    projected = jnp.dot(act[...], ow[...], preferred_element_type=F32).astype(BF16)
    strm[...] = (res[...].astype(F32) + projected.astype(F32)).astype(BF16)

    slot = lax.broadcasted_iota(jnp.int32, (SLOTS, ROWS), 0).astype(F32)
    chosen = ((slot == slots[0]) | (slot == slots[1])).astype(BF16)
    dsp[...] = (
        jnp.dot(chosen, strm[...], preferred_element_type=F32)
        .astype(BF16)
        .reshape(EXPERTS, CAP, LANES)
    )

    own_pos = [
        pl.multiple_of((y * RING + x) * LANES, LANES),
        pl.multiple_of((x * RING + y) * LANES, LANES),
    ]

    def here(r):
        part = PLACE[r][1]
        return x2g.at[pl.ds(r * CAP, CAP), pl.ds(own_pos[part], LANES)]

    for r in range(1, EXPERTS):
        dev = along(-REACH[r // 2], lax.rem(c + r, 2))
        remote(dsp.at[dev[0] * 2 + dev[1]], here(r), dsend, drecv.at[PLACE[r][0] * 2 + PLACE[r][1]], dev).start()
    x2g[:CAP, pl.ds(own_pos[0], LANES)] = dsp[me_sp]

    own2, sets2, relay2, landed2 = make_gather(x2g, rows2, first2, ssem2, rsem2)

    def arrived(g, part):
        rows = rows2(g) - CAP if g + part == 0 else rows2(g)
        ref = x2g.at[pl.ds(first2(g, part), rows), pl.ds(own_pos[part], LANES)]
        pltpu.make_async_copy(ref, ref, drecv.at[g * 2 + part]).wait()
        own2(g, part)

    for w in weights[1:]:
        w.wait()

    def exchange(g, part, kind, src, dst, dev):
        return remote(src, dst, ssem2.at[part, kind], rsem2.at[g, part, kind], dev)

    def expert_stage(g, _):
        landed2(g, 0)
        landed2(g, 1)
        base, count = first2(g, 0), rows2(g)
        for part in range(2):

            def norm_rows(i, carry, part=part):
                lo = pl.multiple_of(base + part * count + i * 16, 16)
                to = pl.multiple_of(part * count + i * 16, 16)
                vals = [
                    x2g[pl.ds(lo, 16), pos * LANES : (pos + 1) * LANES].astype(F32)
                    for pos in range(NTP)
                ]
                total = sum(v * v for v in vals)
                rs = lax.rsqrt(jnp.sum(total, axis=1, keepdims=True) * (1.0 / FULL) + EPS)
                for pos in range(NTP):
                    j = true_block(part, pos)
                    nrm[pl.ds(to, 16), j * LANES : (j + 1) * LANES] = (
                        vals[pos] * rs * gains[1:2, j * LANES : (j + 1) * LANES]
                    ).astype(BF16)
                return carry

            lax.fori_loop(0, count // 16, norm_rows, 0)
        both = pl.ds(0, 2 * count)
        hg = jnp.dot(nrm[both, :], gw[...], preferred_element_type=F32)
        hu = jnp.dot(nrm[both, :], uw[...], preferred_element_type=F32)
        hid[both, :] = ((hg / (1.0 + jnp.exp(-hg))) * hu).astype(BF16)
        for q in range(RING):
            p = jnp.dot(
                hid[both, :], dw[:, q * WIDE : (q + 1) * WIDE], preferred_element_type=F32
            ).astype(BF16)
            part_sum[pl.ds(base, count), q * WIDE : (q + 1) * WIDE] = p[:count, :]
            for i in range(RING):
                at = (i * RING + q) * LANES
                part_sum[pl.ds(base + count, count), at : at + LANES] = p[
                    count:, i * LANES : (i + 1) * LANES
                ]
        for part in range(2):
            _, major, _, wide, _, r = ring(part, g, rows2, first2)
            send(g, part, 6, part_sum.at[r, wide(2)], t1.at[r], major(1))
            send(g, part, 7, part_sum.at[r, wide(-1)], v1.at[r], major(-1))

    def send(g, part, kind, src, dst, dev):
        push(ssem2, part, kind, exchange(g, part, kind, src, dst, dev))

    def pass_on(g, part):
        _, major, _, wide, _, r = ring(part, g, rows2, first2)
        exchange(g, part, 6, t1.at[r], t1.at[r], major(1)).wait_recv()
        s1[r, :] = (t1[r, :].astype(F32) + part_sum[r, wide(1)].astype(F32)).astype(BF16)
        send(g, part, 8, s1.at[r], u1.at[r], major(1))

    def ring_sum(g, part):
        minor, major, _, wide, small, r = ring(part, g, rows2, first2)
        exchange(g, part, 7, v1.at[r], v1.at[r], major(1)).wait_recv()
        exchange(g, part, 8, u1.at[r], u1.at[r], major(1)).wait_recv()
        q1[r, :] = (
            part_sum[r, wide(0)].astype(F32) + u1[r, :].astype(F32) + v1[r, :].astype(F32)
        ).astype(BF16)
        for kind, by, dst in ((9, 1, t2), (10, -1, v2), (11, 2, u2)):
            send(g, part, kind, q1.at[r, small(by)], dst.at[r], minor(by))

    def last_sum(g, part):
        minor, _, _, _, small, r = ring(part, g, rows2, first2)
        total = q1[r, small(0)].astype(F32)
        for kind, dst in ((9, t2), (10, v2), (11, u2)):
            exchange(g, part, kind, dst.at[r], dst.at[r], minor(1)).wait_recv()
        fin[r, :] = (
            total + t2[r, :].astype(F32) + v2[r, :].astype(F32) + u2[r, :].astype(F32)
        ).astype(BF16)
        for i in range(SIZES[g]):
            k = first_chunk(g, part) + i
            if k > 0:
                dev = along(REACH[k // 2], lax.rem(c + k, 2))
                src = fin.at[pl.ds(k * CAP, CAP), :]
                remote(src, ret.at[me_sp], rsend, rrecv, dev).start()

    moves2 = (arrived, sets2, relay2, expert_stage, pass_on, ring_sum, last_sum)
    for code in ORDER:
        moves2[code // 100](code // 10 % 10, code % 10)
    ret[me_sp] = fin[:CAP, :]

    for d in flying.values():
        d.wait_send()

    @pl.when(me_sp < 2 * NZ - 1)
    def _():
        halo_g.wait_send()
        halo_d.wait_send()

    others = ret.at[pl.ds(0, EXPERTS - 1)]
    pltpu.make_async_copy(others, others, dsend).wait()
    pltpu.make_async_copy(others, others, rrecv).wait()
    pltpu.make_async_copy(others, others, rsend).wait()

    back_rows = ret[...].reshape(SLOTS, LANES)
    total = jnp.zeros((ROWS, LANES), F32)
    for k in range(2):
        picked = jnp.dot(pick[k], back_rows, preferred_element_type=F32)
        total = total + picked * to_column(rw[k : k + 1, :])
    out[...] = (strm[...].astype(F32) + total).astype(BF16)


def per_device(
    residual_in,
    conv_value,
    conv_gate,
    doc_ids,
    conv_kernel,
    ln_gain,
    out_weight,
    norm_gain,
    routes,
    route_weight,
    gate_w,
    up_w,
    down_w,
):
    vmem = pl.BlockSpec(memory_space=pltpu.VMEM)
    hbm = pl.BlockSpec(memory_space=pl.ANY)
    dma = pltpu.SemaphoreType.DMA
    hidden = gate_w.shape[2]
    return pl.pallas_call(
        kernel,
        out_shape=jax.ShapeDtypeStruct((ROWS, LANES), BF16),
        in_specs=[hbm] * 13,
        out_specs=vmem,
        scratch_shapes=[
            pltpu.VMEM((FULL, LANES), BF16),
            pltpu.VMEM((FULL, hidden), BF16),
            pltpu.VMEM((FULL, hidden), BF16),
            pltpu.VMEM((hidden, FULL), BF16),
            pltpu.VMEM((HALO + ROWS, LANES), F32),
            pltpu.VMEM((HALO + ROWS, LANES), F32),
            pltpu.VMEM((HALO, LANES), BF16),
            pltpu.VMEM((HALO, LANES), F32),
            pltpu.VMEM((HALO, LANES), BF16),
            pltpu.VMEM((HALO, LANES), F32),
            pltpu.VMEM((ROWS, LANES), F32),
            pltpu.VMEM((NTP, 8, ROWS), F32),
            pltpu.VMEM((8, FULL), F32),
            pltpu.VMEM((ROWS, LANES), F32),
            pltpu.VMEM((ROWS, FULL), BF16),
            pltpu.VMEM((ROWS, FULL), BF16),
            pltpu.VMEM((ROWS, LANES), BF16),
            pltpu.VMEM((2, ROWS, SLOTS), BF16),
            pltpu.VMEM((EXPERTS, CAP, LANES), BF16),
            pltpu.VMEM((SLOTS, FULL), BF16),
            pltpu.VMEM((BIG, FULL), BF16),
            pltpu.VMEM((BIG, hidden), BF16),
            pltpu.VMEM((SLOTS, FULL), BF16),
            pltpu.VMEM((SLOTS, WIDE), BF16),
            pltpu.VMEM((SLOTS, WIDE), BF16),
            pltpu.VMEM((SLOTS, WIDE), BF16),
            pltpu.VMEM((SLOTS, WIDE), BF16),
            pltpu.VMEM((SLOTS, WIDE), BF16),
            pltpu.VMEM((SLOTS, LANES), BF16),
            pltpu.VMEM((SLOTS, LANES), BF16),
            pltpu.VMEM((SLOTS, LANES), BF16),
            pltpu.VMEM((SLOTS, LANES), BF16),
            pltpu.VMEM((SLOTS, LANES), BF16),
            pltpu.VMEM((EXPERTS, CAP, LANES), BF16),
            dma((4,)),
            dma((2,)),
            dma((2,)),
            dma((NTP,)),
            dma((NTP,)),
            dma((2, 6)),
            dma((G1, 2, 6)),
            dma((2, 12)),
            dma((G2, 2, 12)),
            dma(()),
            dma((2 * G2,)),
            dma(()),
            dma(()),
            pltpu.SemaphoreType.REGULAR((4,)),
            pltpu.VMEM((ROWS, LANES), BF16),
            pltpu.VMEM((ROWS, LANES), BF16),
            pltpu.VMEM((1, ROWS), jnp.int32),
            pltpu.VMEM((TAPS, LANES), BF16),
            pltpu.VMEM((1, LANES), BF16),
            pltpu.VMEM((ROWS, LANES), BF16),
            pltpu.VMEM((2, ROWS), jnp.int32),
            pltpu.VMEM((2, ROWS), F32),
            pltpu.VMEM((1, LANES), BF16),
            dma((9,)),
        ],
        compiler_params=pltpu.CompilerParams(
            collective_id=0, has_side_effects=True, vmem_limit_bytes=60 * 1024 * 1024
        ),
        name="layer",
    )(
        conv_value,
        conv_gate,
        doc_ids.reshape(1, ROWS),
        conv_kernel,
        ln_gain.reshape(1, LANES),
        residual_in,
        routes.T,
        route_weight.T,
        norm_gain.reshape(1, LANES),
        out_weight,
        gate_w,
        up_w,
        down_w,
    )


def solution(mesh):
    split = Mesh(mesh.devices.reshape(NZ, 2, RING, RING), AXES)
    in_specs = (
        P(SP, TP),
        P(SP, TP),
        P(SP, TP),
        P(SP),
        P(None, TP),
        P(TP),
        P(None, TP),
        P(TP),
        P(SP, None),
        P(SP, None),
        P(SP, None, TP),
        P(SP, None, TP),
        P(SP, TP, None),
    )
    return jax.shard_map(
        per_device, mesh=split, in_specs=in_specs, out_specs=P(SP, TP), check_vma=False
    )
```

```python
import functools

import jax
import jax.numpy as jnp
from jax import lax
from jax.experimental import pallas as pl
from jax.experimental.pallas import tpu as pltpu
from jax.sharding import Mesh
from jax.sharding import PartitionSpec as P

MESH = pl.DeviceIdType.MESH
F32 = jnp.float32
BF16 = jnp.bfloat16
AXES = ("z", "core", "y", "x")
TP = ("y", "x")
SP = ("z", "core")
EPS = 1e-06

ROWS = 256
LANES = 128
RING = 4
NTP = RING * RING
WIDE = RING * LANES
FULL = NTP * LANES
TAPS = 31
HALO = 32
EXPERTS = 32
CAP = 32
SLOTS = EXPERTS * CAP
NZ = 16
G1 = 2
STEPS1 = (1, -1)
STEPS2 = (1, -1, 1, -1, 1, -1)
R1 = ROWS // G1 // 2
SIZES = (2, 4, 4, 3, 2, 1)
G2 = len(SIZES)
BIG = 2 * max(SIZES) * CAP
REACH = (15, 2, 14, 3, 12, 5, 11, 6, 10, 7, 9, 8, 13, 4, 0, 1)
SELF = 2 * REACH.index(0)
ORDER = (
    0, 1, 10, 11, 100, 101, 20, 21, 110, 111, 200, 201,
    30, 31, 120, 121, 210, 211, 300, 40, 41, 130, 131, 220,
    221, 310, 400, 401, 50, 51, 140, 141, 230, 231, 320, 410,
    411, 500, 501, 150, 151, 240, 241, 330, 420, 421, 510, 511,
    600, 601, 250, 251, 340, 430, 431, 520, 521, 610, 611, 350,
    440, 441, 530, 531, 620, 621, 450, 451, 540, 541, 630, 631,
    550, 551, 640, 641, 650, 651,
)


def remote(src, dst, send, recv, dev):
    return pltpu.make_async_remote_copy(
        src_ref=src,
        dst_ref=dst,
        send_sem=send,
        recv_sem=recv,
        device_id=dev,
        device_id_type=MESH,
    )


def to_column(row):
    return jnp.transpose(jnp.broadcast_to(row, (LANES, row.shape[1])))


def first_chunk(g, part):
    return 2 * sum(SIZES[:g]) + part * SIZES[g]


def first2(g, part):
    return first_chunk(g, part) * CAP


def rows2(g):
    return SIZES[g] * CAP


def rows1(g):
    return R1


PLACE = [(g, p) for g in range(G2) for p in range(2) for _ in range(SIZES[g])]


def true_block(part, pos):
    return pos if part == 0 else (pos % RING) * RING + pos // RING


def kernel(
    cv_hbm,
    cg_hbm,
    doc_hbm,
    ck_hbm,
    lng_hbm,
    res_hbm,
    routes_hbm,
    rw_hbm,
    ng_hbm,
    ow_hbm,
    gw_hbm,
    uw_hbm,
    dw_hbm,
    out,
    ow,
    gw,
    uw,
    dw,
    ext,
    docx,
    hg_out,
    hd_out,
    hg_in,
    hd_in,
    conv,
    stat,
    gains,
    colstat,
    xg,
    act,
    strm,
    pick,
    dsp,
    x2g,
    nrm,
    hid,
    part_sum,
    t1,
    u1,
    v1,
    s1,
    q1,
    t2,
    u2,
    v2,
    s2,
    fin,
    ret,
    wsem,
    hsend,
    hrecv,
    stsend,
    strecv,
    ssem1,
    rsem1,
    ssem2,
    rsem2,
    dsend,
    drecv,
    rsend,
    rrecv,
    ready,
    cv,
    cg,
    doc,
    ck,
    lng,
    res,
    routes,
    rw,
    ng,
    isem,
):
    z = lax.axis_index("z")
    c = lax.axis_index("core")
    y = lax.axis_index("y")
    x = lax.axis_index("x")
    me_tp = y * RING + x
    me_sp = z * 2 + c

    weights = [
        pltpu.make_async_copy(src, dst, wsem.at[i])
        for i, (src, dst) in enumerate(
            ((ow_hbm, ow), (gw_hbm.at[0], gw), (uw_hbm.at[0], uw), (dw_hbm.at[0], dw))
        )
    ]
    small_inputs = [
        pltpu.make_async_copy(src, dst, isem.at[i])
        for i, (src, dst) in enumerate(
            zip(
                (cv_hbm, cg_hbm, doc_hbm, ck_hbm, routes_hbm, lng_hbm, ng_hbm, rw_hbm, res_hbm),
                (cv, cg, doc, ck, routes, lng, ng, rw, res),
            )
        )
    ]
    for w in small_inputs:
        w.start()

    barrier = pltpu.get_barrier_semaphore()

    def tp_peer(k):
        other = lax.rem(me_tp + k, NTP)
        return (z, c, other // RING, lax.rem(other, RING))

    def along(by, core):
        return (lax.rem(z + by + NZ, NZ), core, y, x)

    def tell(sem, dev):
        pl.semaphore_signal(sem, inc=1, device_id=dev, device_id_type=MESH)

    def greet(k, carry):
        tell(barrier, tp_peer(k))
        return carry

    beside = along(2 * c - 1, 1 - c)
    for dev in (along(1, c), along(-1, c), along(0, 1 - c), beside):
        tell(barrier, dev)
    lax.fori_loop(1, NTP, greet, 0)

    for w in weights:
        w.start()
    for w in small_inputs:
        w.wait()

    gate = cg[...].astype(F32)
    gated = (cv[...].astype(F32) * (1.0 / (1.0 + jnp.exp(-gate)))).astype(BF16)
    ext[HALO:, :] = gated.astype(F32)
    hg_out[...] = gated[ROWS - HALO :, :]
    dcol = to_column(doc[...].astype(F32))
    docx[HALO:, :] = dcol
    hd_out[...] = dcol[ROWS - HALO :, :]
    taps = ck[...].astype(F32)

    def conv_rows(first, count):
        acc = jnp.zeros((count, LANES), F32)
        mine = docx[HALO + first : HALO + first + count, :]
        for tap in range(TAPS):
            at = HALO + first - (TAPS - 1) + tap
            same = docx[at : at + count, :] == mine
            term = ext[at : at + count, :] * taps[tap : tap + 1, :]
            acc = acc + jnp.where(same, term, 0.0)
        conv[first : first + count, :] = acc

    for first in range(HALO, ROWS, 32):
        conv_rows(first, 32)

    pl.semaphore_wait(barrier, NTP - 1 + 4)

    def spread_word(i):
        if i > 0:
            pl.semaphore_wait(ready.at[i - 1], 1 if i == 1 else 2)
        if i == 0:
            tell(ready.at[0], along(0, 1 - c))
        elif i < 4:
            for by in (1 << (i - 1), -(1 << (i - 1))):
                tell(ready.at[i], along(by, c))

    spread_word(0)
    after = along(c, 1 - c)
    halo_g = remote(hg_out, hg_in, hsend.at[0], hrecv.at[0], after)
    halo_d = remote(hd_out, hd_in, hsend.at[1], hrecv.at[1], after)

    @pl.when(me_sp < 2 * NZ - 1)
    def _():
        halo_g.start()
        halo_d.start()

    ids = routes[...]
    expert = lax.broadcasted_iota(jnp.int32, (EXPERTS, ROWS), 0)
    names = [(expert == ids[k : k + 1, :]).astype(F32) for k in range(2)]
    before = (
        lax.broadcasted_iota(jnp.int32, (ROWS, ROWS), 0)
        < lax.broadcasted_iota(jnp.int32, (ROWS, ROWS), 1)
    ).astype(F32)
    earlier = jnp.dot(
        (names[0] + names[1]).astype(BF16), before.astype(BF16), preferred_element_type=F32
    )
    slot_base = expert.astype(F32) * float(CAP)
    slots = [jnp.sum(n * (earlier + slot_base), axis=0, keepdims=True) for n in names]
    lane = lax.broadcasted_iota(jnp.int32, (ROWS, LANES), 1).astype(F32)
    for k in range(2):
        col = to_column(slots[k])
        for b in range(SLOTS // LANES):
            pick[k, :, b * LANES : (b + 1) * LANES] = (
                (lane + float(b * LANES)) == col
            ).astype(BF16)

    first_block = me_sp == 0

    @pl.when(me_sp > 0)
    def _():
        halo_g.wait_recv()
        halo_d.wait_recv()

    spread_word(1)
    ext[:HALO, :] = jnp.where(first_block, 0.0, hg_in[...].astype(F32))
    docx[:HALO, :] = jnp.where(first_block, -1.0, hd_in[...])
    conv_rows(0, HALO)

    cx = conv[...]
    cxt = jnp.transpose(cx)
    local = jnp.sum(cxt, axis=0, keepdims=True) * (1.0 / LANES)
    spread = cxt - local
    second = jnp.sum(spread * spread, axis=0, keepdims=True)
    gain_row = jnp.concatenate([lng[...].astype(F32), ng[...].astype(F32)], axis=1)
    stat[me_tp] = jnp.concatenate(
        [local, second, gain_row, jnp.zeros((5, ROWS), F32)], axis=0
    )
    dev = (cx - to_column(local)).astype(BF16)
    for g in range(G1):
        for part in range(2):
            mm, mj = (x, y) if part == 0 else (y, x)
            lo = g * 2 * R1 + part * R1
            pos = pl.multiple_of((mj * RING + mm) * LANES, LANES)
            xg[lo : lo + R1, pl.ds(pos, LANES)] = dev[lo : lo + R1, :]

    def send_stat(k, carry):
        remote(stat.at[me_tp], stat.at[me_tp], stsend.at[k], strecv.at[k], tp_peer(k)).start()
        return carry

    def ring(part, g, rows, first, steps):
        mm, mj = (x, y) if part == 0 else (y, x)
        step = steps[g]

        def at(base, by):
            return lax.rem(base + by * step + 2 * RING, RING)

        def minor(by):
            m = at(mm, by)
            return (z, c, mj, m) if part == 0 else (z, c, m, mj)

        def major(by):
            m = at(mj, by)
            return (z, c, m, mm) if part == 0 else (z, c, mm, m)

        def block(by):
            return pl.ds(pl.multiple_of((mj * RING + at(mm, by)) * LANES, LANES), LANES)

        def wide(by):
            return pl.ds(pl.multiple_of(at(mj, by) * WIDE, WIDE), WIDE)

        def small(by):
            return pl.ds(pl.multiple_of(at(mm, by) * LANES, LANES), LANES)

        return minor, major, block, wide, small, pl.ds(first(g, part), rows(g))

    flying = {}

    def push(ssem, part, kind, d):
        key = (id(ssem), part, kind)
        if key in flying:
            flying[key].wait_send()
        d.start()
        flying[key] = d

    def make_gather(buf, rows, first, steps, ssem, rsem):
        def move(g, part, kind, cols, dev):
            ref = buf.at[pl.ds(first(g, part), rows(g)), cols]
            return remote(ref, ref, ssem.at[part, kind], rsem.at[g, part, kind], dev)

        def own(g, part):
            minor, _, block, _, _, _ = ring(part, g, rows, first, steps)
            for kind, by in enumerate((1, -1, 2)):
                push(ssem, part, kind, move(g, part, kind, block(0), minor(by)))

        def sets(g, part):
            minor, major, block, wide, _, _ = ring(part, g, rows, first, steps)
            for kind, by in enumerate((-1, 1, 2)):
                move(g, part, kind, block(by), minor(1)).wait_recv()
            push(ssem, part, 3, move(g, part, 3, wide(0), major(1)))
            push(ssem, part, 4, move(g, part, 4, wide(0), major(-1)))

        def relay(g, part):
            _, major, _, wide, _, _ = ring(part, g, rows, first, steps)
            move(g, part, 3, wide(-1), major(1)).wait_recv()
            push(ssem, part, 5, move(g, part, 5, wide(-1), major(1)))

        def landed(g, part):
            _, major, _, wide, _, _ = ring(part, g, rows, first, steps)
            move(g, part, 4, wide(1), major(1)).wait_recv()
            move(g, part, 5, wide(2), major(1)).wait_recv()

        return own, sets, relay, landed

    def first1(g, part):
        return g * 2 * R1 + part * R1

    own1, sets1, relay1, landed1 = make_gather(xg, rows1, first1, STEPS1, ssem1, rsem1)
    moves1 = [(g, part) for g in range(G1) for part in range(2)]
    for g, part in moves1:
        own1(g, part)
    lax.fori_loop(1, NTP, send_stat, 0)
    spread_word(2)
    for g, part in moves1:
        sets1(g, part)
    spread_word(3)

    def wait_stat(k, carry):
        d = remote(stat.at[me_tp], stat.at[me_tp], stsend.at[k], strecv.at[k], tp_peer(k))
        d.wait_send()
        d.wait_recv()
        return carry

    for g, part in moves1:
        relay1(g, part)
    lax.fori_loop(1, NTP, wait_stat, 0)

    means = [stat[j, 0:1, :] for j in range(NTP)]
    mean = sum(means) * (1.0 / NTP)
    shifts = [m - mean for m in means]
    var = (
        sum(stat[j, 1:2, :] for j in range(NTP)) * (1.0 / FULL)
        + sum(s * s for s in shifts) * (1.0 / NTP)
    )
    scale = lax.rsqrt(var + EPS)
    table = jnp.concatenate(shifts + [scale] + [jnp.zeros((LANES - NTP - 1, ROWS), F32)], axis=0)
    colstat[...] = jnp.transpose(table)
    for j in range(NTP):
        gains[:, j * LANES : (j + 1) * LANES] = jnp.concatenate(
            [stat[j, 2:3, :LANES], stat[j, 2:3, LANES:], jnp.zeros((6, LANES), F32)], axis=0
        )

    def normalise(g, part):
        landed1(g, part)

        def some(i, carry):
            lo = pl.multiple_of(first1(g, part) + i * 16, 16)
            cs = colstat[pl.ds(lo, 16), :]
            rs = cs[:, NTP : NTP + 1]
            for pos in range(NTP):
                j = true_block(part, pos)
                v = xg[pl.ds(lo, 16), pos * LANES : (pos + 1) * LANES].astype(F32)
                v = (v + cs[:, j : j + 1]) * rs * gains[0:1, j * LANES : (j + 1) * LANES]
                v = v / (1.0 + jnp.exp(-v))
                act[pl.ds(lo, 16), j * LANES : (j + 1) * LANES] = v.astype(BF16)
            return carry

        lax.fori_loop(0, R1 // 16, some, 0)

    for g, part in moves1:
        normalise(g, part)
    spread_word(4)

    weights[0].wait()
    projected = jnp.dot(act[...], ow[...], preferred_element_type=F32).astype(BF16)
    strm[...] = (res[...].astype(F32) + projected.astype(F32)).astype(BF16)

    slot = lax.broadcasted_iota(jnp.int32, (SLOTS, ROWS), 0).astype(F32)
    chosen = ((slot == slots[0]) | (slot == slots[1])).astype(BF16)
    dsp[...] = (
        jnp.dot(chosen, strm[...], preferred_element_type=F32)
        .astype(BF16)
        .reshape(EXPERTS, CAP, LANES)
    )

    own_pos = [
        pl.multiple_of((y * RING + x) * LANES, LANES),
        pl.multiple_of((x * RING + y) * LANES, LANES),
    ]

    def here(r):
        part = PLACE[r][1]
        return x2g.at[pl.ds(r * CAP, CAP), pl.ds(own_pos[part], LANES)]

    for r in (*range(SELF), *range(SELF + 1, EXPERTS)):
        dev = along(-REACH[r // 2], lax.rem(c + r, 2))
        remote(dsp.at[dev[0] * 2 + dev[1]], here(r), dsend, drecv.at[PLACE[r][0] * 2 + PLACE[r][1]], dev).start()
    x2g[SELF * CAP : (SELF + 1) * CAP, pl.ds(own_pos[PLACE[SELF][1]], LANES)] = dsp[me_sp]

    own2, sets2, relay2, landed2 = make_gather(x2g, rows2, first2, STEPS2, ssem2, rsem2)

    def arrived(g, part):
        less = CAP if (g, part) == PLACE[SELF] else 0
        ref = x2g.at[
            pl.ds(first2(g, part) + less, rows2(g) - less), pl.ds(own_pos[part], LANES)
        ]
        pltpu.make_async_copy(ref, ref, drecv.at[g * 2 + part]).wait()
        own2(g, part)

    for w in weights[1:]:
        w.wait()

    def exchange(g, part, kind, src, dst, dev):
        return remote(src, dst, ssem2.at[part, kind], rsem2.at[g, part, kind], dev)

    def expert_stage(g, _):
        landed2(g, 0)
        landed2(g, 1)
        base, count = first2(g, 0), rows2(g)
        for part in range(2):

            def norm_rows(i, carry, part=part):
                lo = pl.multiple_of(base + part * count + i * 16, 16)
                to = pl.multiple_of(part * count + i * 16, 16)
                vals = [
                    x2g[pl.ds(lo, 16), pos * LANES : (pos + 1) * LANES].astype(F32)
                    for pos in range(NTP)
                ]
                total = sum(v * v for v in vals)
                rs = lax.rsqrt(jnp.sum(total, axis=1, keepdims=True) * (1.0 / FULL) + EPS)
                for pos in range(NTP):
                    j = true_block(part, pos)
                    nrm[pl.ds(to, 16), j * LANES : (j + 1) * LANES] = (
                        vals[pos] * rs * gains[1:2, j * LANES : (j + 1) * LANES]
                    ).astype(BF16)
                return carry

            lax.fori_loop(0, count // 16, norm_rows, 0)
        both = pl.ds(0, 2 * count)
        hg = jnp.dot(nrm[both, :], gw[...], preferred_element_type=F32)
        hu = jnp.dot(nrm[both, :], uw[...], preferred_element_type=F32)
        hid[both, :] = ((hg / (1.0 + jnp.exp(-hg))) * hu).astype(BF16)
        for q in range(RING):
            p = jnp.dot(
                hid[both, :], dw[:, q * WIDE : (q + 1) * WIDE], preferred_element_type=F32
            ).astype(BF16)
            part_sum[pl.ds(base, count), q * WIDE : (q + 1) * WIDE] = p[:count, :]
            for i in range(RING):
                at = (i * RING + q) * LANES
                part_sum[pl.ds(base + count, count), at : at + LANES] = p[
                    count:, i * LANES : (i + 1) * LANES
                ]
        for part in range(2):
            _, major, _, wide, _, r = ring(part, g, rows2, first2, STEPS2)
            send(g, part, 6, part_sum.at[r, wide(2)], t1.at[r], major(1))
            send(g, part, 7, part_sum.at[r, wide(-1)], v1.at[r], major(-1))

    def send(g, part, kind, src, dst, dev):
        push(ssem2, part, kind, exchange(g, part, kind, src, dst, dev))

    def pass_on(g, part):
        _, major, _, wide, _, r = ring(part, g, rows2, first2, STEPS2)
        exchange(g, part, 6, t1.at[r], t1.at[r], major(1)).wait_recv()
        s1[r, :] = (t1[r, :].astype(F32) + part_sum[r, wide(1)].astype(F32)).astype(BF16)
        send(g, part, 8, s1.at[r], u1.at[r], major(1))

    def ring_sum(g, part):
        minor, major, _, wide, small, r = ring(part, g, rows2, first2, STEPS2)
        exchange(g, part, 7, v1.at[r], v1.at[r], major(1)).wait_recv()
        exchange(g, part, 8, u1.at[r], u1.at[r], major(1)).wait_recv()
        q1[r, :] = (
            part_sum[r, wide(0)].astype(F32) + u1[r, :].astype(F32) + v1[r, :].astype(F32)
        ).astype(BF16)
        for kind, by, dst in ((9, 1, t2), (10, -1, v2), (11, 2, u2)):
            send(g, part, kind, q1.at[r, small(by)], dst.at[r], minor(by))

    def last_sum(g, part):
        minor, _, _, _, small, r = ring(part, g, rows2, first2, STEPS2)
        total = q1[r, small(0)].astype(F32)
        for kind, dst in ((9, t2), (10, v2), (11, u2)):
            exchange(g, part, kind, dst.at[r], dst.at[r], minor(1)).wait_recv()
        fin[r, :] = (
            total + t2[r, :].astype(F32) + v2[r, :].astype(F32) + u2[r, :].astype(F32)
        ).astype(BF16)
        for i in range(SIZES[g]):
            k = first_chunk(g, part) + i
            if k != SELF:
                dev = along(REACH[k // 2], lax.rem(c + k, 2))
                src = fin.at[pl.ds(k * CAP, CAP), :]
                remote(src, ret.at[me_sp], rsend, rrecv, dev).start()

    moves2 = (arrived, sets2, relay2, expert_stage, pass_on, ring_sum, last_sum)
    for code in ORDER:
        moves2[code // 100](code // 10 % 10, code % 10)
    ret[me_sp] = fin[SELF * CAP : (SELF + 1) * CAP, :]

    for d in flying.values():
        d.wait_send()

    @pl.when(me_sp < 2 * NZ - 1)
    def _():
        halo_g.wait_send()
        halo_d.wait_send()

    others = ret.at[pl.ds(0, EXPERTS - 1)]
    pltpu.make_async_copy(others, others, dsend).wait()
    pltpu.make_async_copy(others, others, rrecv).wait()
    pltpu.make_async_copy(others, others, rsend).wait()

    back_rows = ret[...].reshape(SLOTS, LANES)
    total = jnp.zeros((ROWS, LANES), F32)
    for k in range(2):
        picked = jnp.dot(pick[k], back_rows, preferred_element_type=F32)
        total = total + picked * to_column(rw[k : k + 1, :])
    out[...] = (strm[...].astype(F32) + total).astype(BF16)


def per_device(
    residual_in,
    conv_value,
    conv_gate,
    doc_ids,
    conv_kernel,
    ln_gain,
    out_weight,
    norm_gain,
    routes,
    route_weight,
    gate_w,
    up_w,
    down_w,
):
    vmem = pl.BlockSpec(memory_space=pltpu.VMEM)
    hbm = pl.BlockSpec(memory_space=pl.ANY)
    dma = pltpu.SemaphoreType.DMA
    hidden = gate_w.shape[2]
    return pl.pallas_call(
        kernel,
        out_shape=jax.ShapeDtypeStruct((ROWS, LANES), BF16),
        in_specs=[hbm] * 13,
        out_specs=vmem,
        scratch_shapes=[
            pltpu.VMEM((FULL, LANES), BF16),
            pltpu.VMEM((FULL, hidden), BF16),
            pltpu.VMEM((FULL, hidden), BF16),
            pltpu.VMEM((hidden, FULL), BF16),
            pltpu.VMEM((HALO + ROWS, LANES), F32),
            pltpu.VMEM((HALO + ROWS, LANES), F32),
            pltpu.VMEM((HALO, LANES), BF16),
            pltpu.VMEM((HALO, LANES), F32),
            pltpu.VMEM((HALO, LANES), BF16),
            pltpu.VMEM((HALO, LANES), F32),
            pltpu.VMEM((ROWS, LANES), F32),
            pltpu.VMEM((NTP, 8, ROWS), F32),
            pltpu.VMEM((8, FULL), F32),
            pltpu.VMEM((ROWS, LANES), F32),
            pltpu.VMEM((ROWS, FULL), BF16),
            pltpu.VMEM((ROWS, FULL), BF16),
            pltpu.VMEM((ROWS, LANES), BF16),
            pltpu.VMEM((2, ROWS, SLOTS), BF16),
            pltpu.VMEM((EXPERTS, CAP, LANES), BF16),
            pltpu.VMEM((SLOTS, FULL), BF16),
            pltpu.VMEM((BIG, FULL), BF16),
            pltpu.VMEM((BIG, hidden), BF16),
            pltpu.VMEM((SLOTS, FULL), BF16),
            pltpu.VMEM((SLOTS, WIDE), BF16),
            pltpu.VMEM((SLOTS, WIDE), BF16),
            pltpu.VMEM((SLOTS, WIDE), BF16),
            pltpu.VMEM((SLOTS, WIDE), BF16),
            pltpu.VMEM((SLOTS, WIDE), BF16),
            pltpu.VMEM((SLOTS, LANES), BF16),
            pltpu.VMEM((SLOTS, LANES), BF16),
            pltpu.VMEM((SLOTS, LANES), BF16),
            pltpu.VMEM((SLOTS, LANES), BF16),
            pltpu.VMEM((SLOTS, LANES), BF16),
            pltpu.VMEM((EXPERTS, CAP, LANES), BF16),
            dma((4,)),
            dma((2,)),
            dma((2,)),
            dma((NTP,)),
            dma((NTP,)),
            dma((2, 6)),
            dma((G1, 2, 6)),
            dma((2, 12)),
            dma((G2, 2, 12)),
            dma(()),
            dma((2 * G2,)),
            dma(()),
            dma(()),
            pltpu.SemaphoreType.REGULAR((4,)),
            pltpu.VMEM((ROWS, LANES), BF16),
            pltpu.VMEM((ROWS, LANES), BF16),
            pltpu.VMEM((1, ROWS), jnp.int32),
            pltpu.VMEM((TAPS, LANES), BF16),
            pltpu.VMEM((1, LANES), BF16),
            pltpu.VMEM((ROWS, LANES), BF16),
            pltpu.VMEM((2, ROWS), jnp.int32),
            pltpu.VMEM((2, ROWS), F32),
            pltpu.VMEM((1, LANES), BF16),
            dma((9,)),
        ],
        compiler_params=pltpu.CompilerParams(
            collective_id=0, has_side_effects=True, vmem_limit_bytes=60 * 1024 * 1024
        ),
        name="layer",
    )(
        conv_value,
        conv_gate,
        doc_ids.reshape(1, ROWS),
        conv_kernel,
        ln_gain.reshape(1, LANES),
        residual_in,
        routes.T,
        route_weight.T,
        norm_gain.reshape(1, LANES),
        out_weight,
        gate_w,
        up_w,
        down_w,
    )


def solution(mesh):
    split = Mesh(mesh.devices.reshape(NZ, 2, RING, RING), AXES)
    in_specs = (
        P(SP, TP),
        P(SP, TP),
        P(SP, TP),
        P(SP),
        P(None, TP),
        P(TP),
        P(None, TP),
        P(TP),
        P(SP, None),
        P(SP, None),
        P(SP, None, TP),
        P(SP, None, TP),
        P(SP, TP, None),
    )
    return jax.shard_map(
        per_device, mesh=split, in_specs=in_specs, out_specs=P(SP, TP), check_vma=False
    )
```
